32 devices in a mesh: sp: 8 (over z, y), tp: 4 (over x, core).
Axes of the slice: x: 2, y: 2, z: 4, core: 2. Of those that a mesh axis runs over, the one named last changes fastest.
Arguments:
- residual: bfloat16 [5120, 2048], P(('sp', 'tp')), may hold values from -6 to 6
- small_value_inputs: bfloat16 [5120, 1024], P('sp', 'tp'), may hold values from -6 to 6
- large_value_inputs: bfloat16 [5120, 1024], P('sp', 'tp'), may hold values from -6 to 6
- small_gate_inputs: bfloat16 [5120, 1024], P('sp', 'tp'), may hold values from -6 to 6
- large_gate_inputs: bfloat16 [5120, 1024], P('sp', 'tp'), may hold values from -6 to 6
- state_projections: bfloat16 [5120, 4, 128], P('sp'), may hold values from -6 to 6
- small_step_inputs: bfloat16 [5120, 16], P('sp', 'tp'), may hold values from -2.5 to 2.5
- large_step_inputs: bfloat16 [5120, 8], P('sp', 'tp'), may hold values from -2.5 to 2.5
- small_decay_offsets: float32 [5120, 16], P('sp', 'tp'), may hold values from -1.4 to 0
- large_decay_offsets: float32 [5120, 8], P('sp', 'tp'), may hold values from -1.4 to 0
- small_decay_rates: float32 [16], P('tp'), may hold values from -11.1 to -3.1
- large_decay_rates: float32 [8], P('tp'), may hold values from -11.1 to -3.1
- small_filter_taps: bfloat16 [4, 1024], P(None, 'tp'), may hold values from -3 to 3
- large_filter_taps: bfloat16 [4, 1024], P(None, 'tp'), may hold values from -3 to 3
- state_filter_taps: bfloat16 [4, 4, 128], replicated, may hold values from -3 to 3
- small_head_gains: float32 [1024], P('tp'), may hold values from 0.1 to 1.9
- large_head_gains: float32 [1024], P('tp'), may hold values from 0.1 to 1.9
- small_output_projection: bfloat16 [1024, 2048], P('tp'), may hold values from -0.125 to 0.125
- large_output_projection: bfloat16 [1024, 2048], P('tp'), may hold values from -0.125 to 0.125
- channel_norm_gain: float32 [2048], replicated, may hold values from 0.1 to 1.9
- gate_matrix: bfloat16 [2048, 5632], P('sp', 'tp'), may hold values from -0.125 to 0.125
- up_matrix: bfloat16 [2048, 5632], P('sp', 'tp'), may hold values from -0.125 to 0.125
- down_matrix: bfloat16 [5632, 2048], P('tp', 'sp'), may hold values from -0.078125 to 0.078125
Outputs:
- layer_out: bfloat16 [5120, 2048], P(('sp', 'tp'))
The draws below stay inside these ranges and needn't reach their ends.
All inputs are finite; a program needn't handle non-finite values.
Results may differ from the reference program's by a relative error of at most 0.015.
Values may be sent and summed in bfloat16 or wider, within the bound.
A program may use at most 64 MiB of HBM per device.

```python
import jax
import jax.numpy as jnp
from jax import lax

D = 2048
FF = 5632
SMALL_HEADS = 16
LARGE_HEADS = 8
STATE = 128
BLOCK = 64
CONV = 4
TOK_DEV = 640
TOKENS = 5120
W1 = 1024
W2 = 1024
N_TP = 4


def step_draw(key, head_outputs):
    first, second = jax.random.split(key)
    blocks = TOKENS // TOK_DEV
    offset = jax.random.uniform(first, (blocks, 1, head_outputs), jnp.float32, -1.0, 1.0)
    base = 0.5 * jax.random.truncated_normal(second, -3.0, 3.0, (blocks, TOK_DEV, head_outputs), jnp.float32)
    return (base + offset).reshape(TOKENS, head_outputs).astype(jnp.bfloat16)


def rate_draw(key, head_outputs):
    first, second, third = jax.random.split(key, 3)
    quick = jax.random.uniform(first, (head_outputs,), jnp.float32) < 0.5
    slow_rate = jax.random.uniform(second, (head_outputs,), jnp.float32, 0.2, 0.8) / (0.75 * TOKENS)
    fast_rate = 1.0 / (0.75 * jax.random.uniform(third, (head_outputs,), jnp.float32, 30.0, 100.0))
    return jnp.log(jnp.where(quick, fast_rate, slow_rate)).astype(jnp.float32)


def decay_offset_sample(key, head_outputs):
    first, second = jax.random.split(key)
    places = jax.random.randint(first, (2, head_outputs), 0, TOKENS)
    sizes = jnp.log(jax.random.uniform(second, (2, head_outputs), jnp.float32, 0.5, 0.8))
    hit = jnp.arange(TOKENS, dtype=jnp.int32)[:, None, None] == places[None, :, :]
    return jnp.sum(jnp.where(hit, sizes[None, :, :], 0.0), axis=1).astype(jnp.float32)


def draw_small_step_inputs(key, part):
    return step_draw(jax.random.fold_in(key, 11), SMALL_HEADS)


def draw_large_step_inputs(key, part):
    return step_draw(jax.random.fold_in(key, 12), LARGE_HEADS)


def draw_small_decay_rates(key, part):
    return rate_draw(jax.random.fold_in(key, 21), SMALL_HEADS)


def draw_large_decay_rates(key, part):
    return rate_draw(jax.random.fold_in(key, 22), LARGE_HEADS)


def draw_small_decay_offsets(key, part):
    return decay_offset_sample(jax.random.fold_in(key, 31), SMALL_HEADS)


def draw_large_decay_offsets(key, part):
    return decay_offset_sample(jax.random.fold_in(key, 32), LARGE_HEADS)


def steps_of(own_key, dims, cuts, low, largest):
    level = 1.0
    for position, blocks in cuts:
        heights = jax.random.uniform(jax.random.fold_in(jax.random.fold_in(own_key, 6), position), (blocks,), jnp.float32, low / len(cuts), largest / len(cuts))
        level = level * jnp.repeat(jnp.exp(heights), dims[position] // blocks).reshape((-1,) + (1,) * (len(dims) - 1 - position))
    return level


def normal_values(stream_key, shape, scale, bound, cuts=(), kind=jnp.bfloat16):
    result = jax.random.normal(stream_key, shape, jnp.float32) * scale
    if len(cuts) > 0:
        result = steps_of(stream_key, shape, cuts, -0.22, 0.18) * result
    return jnp.clip(result, min=-bound, max=bound).astype(kind)


def setup_inputs(seed: int = 0) -> dict:
    arg_keys = jax.random.split(jax.random.key(seed), 24)
    return {
        "residual": normal_values(arg_keys[0], (TOKENS, D), 1.0, 6.0, ((0, 32),)),
        "small_value_inputs": normal_values(arg_keys[1], (TOKENS, W1), 1.0, 6.0, ((0, 8), (1, 4))),
        "large_value_inputs": normal_values(arg_keys[2], (TOKENS, W2), 1.0, 6.0, ((0, 8), (1, 4))),
        "small_gate_inputs": normal_values(arg_keys[3], (TOKENS, W1), 1.0, 6.0, ((0, 8), (1, 4))),
        "large_gate_inputs": normal_values(arg_keys[4], (TOKENS, W2), 1.0, 6.0, ((0, 8), (1, 4))),
        "state_projections": normal_values(arg_keys[5], (TOKENS, 4, STATE), 1.0, 6.0, ((0, 8),)),
        "small_step_inputs": draw_small_step_inputs(jax.random.fold_in(arg_keys[23], 71), 0),
        "large_step_inputs": draw_large_step_inputs(jax.random.fold_in(arg_keys[23], 71), 0),
        "small_decay_offsets": draw_small_decay_offsets(jax.random.fold_in(arg_keys[23], 71), 0),
        "large_decay_offsets": draw_large_decay_offsets(jax.random.fold_in(arg_keys[23], 71), 0),
        "small_decay_rates": draw_small_decay_rates(jax.random.fold_in(arg_keys[23], 71), 0),
        "large_decay_rates": draw_large_decay_rates(jax.random.fold_in(arg_keys[23], 71), 0),
        "small_filter_taps": normal_values(arg_keys[12], (CONV, W1), CONV ** -0.5, 3.0, ((1, 4),)),
        "large_filter_taps": normal_values(arg_keys[13], (CONV, W2), CONV ** -0.5, 3.0, ((1, 4),)),
        "state_filter_taps": normal_values(arg_keys[14], (CONV, 4, STATE), CONV ** -0.5, 3.0),
        "small_head_gains": jnp.clip(1.0 + 0.18 * jax.random.normal(arg_keys[15], (W1,), jnp.float32), 0.1, 1.9),
        "large_head_gains": jnp.clip(1.0 + 0.18 * jax.random.normal(arg_keys[16], (W2,), jnp.float32), 0.1, 1.9),
        "small_output_projection": normal_values(arg_keys[17], (W1, D), (W1 + W2) ** -0.5, 0.125, ((0, 4),)),
        "large_output_projection": normal_values(arg_keys[18], (W2, D), (W1 + W2) ** -0.5, 0.125, ((0, 4),)),
        "channel_norm_gain": jnp.clip(1.0 + 0.18 * jax.random.normal(arg_keys[19], (D,), jnp.float32), 0.1, 1.9),
        "gate_matrix": normal_values(arg_keys[20], (D, FF), D ** -0.5, 0.125, ((0, 8), (1, 4))),
        "up_matrix": normal_values(arg_keys[21], (D, FF), D ** -0.5, 0.125, ((0, 8), (1, 4))),
        "down_matrix": normal_values(arg_keys[22], (FF, D), FF ** -0.5, 0.078125, ((0, 4), (1, 8))),
    }


HIGH = lax.Precision.HIGHEST
head_eps = 1e-05
row_eps = 1e-06

def rounded(value):
    return lax.optimization_barrier(value.astype(jnp.bfloat16)).astype(jnp.float32)

def causal_conv(series, prior_tokens, filter_taps):
    width = filter_taps.shape[0]
    length = series.shape[0]
    padded = jnp.concatenate([prior_tokens.astype(jnp.float32), series.astype(jnp.float32)], axis=0)
    total = jnp.zeros(series.shape, jnp.float32)
    for offset in range(width):
        total = total + filter_taps[offset].astype(jnp.float32)[None, :] * padded[offset:offset + length]
    return jax.nn.silu(total)

def block_scan(driven, decay_logarithm, key_vectors, read_vectors, state):
    length, head_outputs, size = driven.shape
    blocks = length // BLOCK
    mask = jnp.tril(jnp.ones((BLOCK, BLOCK), dtype=bool))[:, :, None]

    def advance(carry, pieces):
        values, decays, key_rows, read_rows = pieces
        within = jnp.cumsum(decays, axis=0)
        spread = within[:, None, :] - within[None, :, :]
        weights = jnp.where(mask, jnp.exp(jnp.where(mask, spread, 0.0)), 0.0)
        scores = jnp.dot(read_rows, key_rows.T, precision=HIGH)
        inner = jnp.einsum('ls,lsh,shp->lhp', scores, weights, values, precision=HIGH)
        carried = jnp.einsum('ln,hpn,lh->lhp', read_rows, carry, jnp.exp(within), precision=HIGH)
        tail = jnp.exp(within[-1][None, :] - within)
        fresh = jnp.einsum('ln,lh,lhp->hpn', key_rows, tail, values, precision=HIGH)
        return (carry * jnp.exp(within[-1])[:, None, None] + fresh, inner + carried)
    pieces = (driven.reshape(blocks, BLOCK, head_outputs, size), decay_logarithm.reshape(blocks, BLOCK, head_outputs), key_vectors.reshape(blocks, BLOCK, key_vectors.shape[1]), read_vectors.reshape(blocks, BLOCK, read_vectors.shape[1]))
    final, outs = lax.scan(advance, state, pieces)
    return (final, outs.reshape(length, head_outputs, size))

def heads_per_group(input_rows, gate_inputs, step_inputs, decay_offsets, decay_rates, filter_taps, head_gains, key_vectors, read_vectors):
    length, width = input_rows.shape
    head_outputs = decay_rates.shape[0]
    size = width // head_outputs
    prior_tokens = jnp.zeros((filter_taps.shape[0] - 1, width), jnp.bfloat16)
    conv_values = causal_conv(input_rows, prior_tokens, filter_taps)
    step_amount = jax.nn.softplus(step_inputs.astype(jnp.float32))
    decay_logarithm = -jnp.exp(decay_rates)[None, :] * step_amount + decay_offsets
    driven = conv_values.reshape(length, head_outputs, size) * step_amount[:, :, None]
    start_state = jnp.zeros((head_outputs, size, key_vectors.shape[1]), jnp.float32)
    _, scan_out = block_scan(driven, decay_logarithm, key_vectors, read_vectors, start_state)
    gated = scan_out * jax.nn.silu(gate_inputs.reshape(length, head_outputs, size).astype(jnp.float32))
    scale = lax.rsqrt(lax.optimization_barrier(jnp.mean(gated * gated, axis=-1, keepdims=True)) + head_eps)
    normed = gated * scale * head_gains.reshape(head_outputs, size).astype(jnp.float32)
    return normed.reshape(length, width).astype(jnp.bfloat16)

def row_norm(rows, gain):
    wide = rows.astype(jnp.float32)
    scale = lax.rsqrt(lax.optimization_barrier(jnp.mean(wide * wide, axis=-1, keepdims=True)) + row_eps)
    return (wide * scale * gain[None, :]).astype(jnp.bfloat16)

def reference(residual, small_value_inputs, large_value_inputs, small_gate_inputs, large_gate_inputs, state_projections, small_step_inputs, large_step_inputs, small_decay_offsets, large_decay_offsets, small_decay_rates, large_decay_rates, small_filter_taps, large_filter_taps, state_filter_taps, small_head_gains, large_head_gains, small_output_projection, large_output_projection, channel_norm_gain, gate_matrix, up_matrix, down_matrix):
    length = residual.shape[0]
    planes = state_projections.shape[1] * state_projections.shape[2]
    flat = state_projections.reshape(length, planes)
    flat_taps = state_filter_taps.reshape(state_filter_taps.shape[0], planes)
    prior_tokens = jnp.zeros((state_filter_taps.shape[0] - 1, planes), jnp.bfloat16)
    convolved_state_maps = causal_conv(flat, prior_tokens, flat_taps).reshape(length, state_projections.shape[1], state_projections.shape[2])
    small_head_outputs = heads_per_group(small_value_inputs, small_gate_inputs, small_step_inputs, small_decay_offsets, small_decay_rates, small_filter_taps, small_head_gains, convolved_state_maps[:, 0], convolved_state_maps[:, 1])
    large_head_outputs = heads_per_group(large_value_inputs, large_gate_inputs, large_step_inputs, large_decay_offsets, large_decay_rates, large_filter_taps, large_head_gains, convolved_state_maps[:, 2], convolved_state_maps[:, 3])
    slice_small = W1 // N_TP
    slice_large = W2 // N_TP
    mixed = jnp.zeros((length, D), jnp.float32)
    for part in range(N_TP):
        term = jnp.dot(small_head_outputs[:, part * slice_small:(part + 1) * slice_small], small_output_projection[part * slice_small:(part + 1) * slice_small], preferred_element_type=jnp.float32)
        term = term + jnp.dot(large_head_outputs[:, part * slice_large:(part + 1) * slice_large], large_output_projection[part * slice_large:(part + 1) * slice_large], preferred_element_type=jnp.float32)
        mixed = mixed + rounded(term)
    middle = (residual.astype(jnp.float32) + mixed).astype(jnp.bfloat16)
    normed = row_norm(middle, channel_norm_gain)
    gate = jnp.dot(normed, gate_matrix, preferred_element_type=jnp.float32)
    up = jnp.dot(normed, up_matrix, preferred_element_type=jnp.float32)
    hidden = (jax.nn.silu(gate) * up).astype(jnp.bfloat16)
    slice_units = FF // N_TP
    down = jnp.zeros((length, D), jnp.float32)
    for part in range(N_TP):
        down = down + rounded(jnp.dot(hidden[:, part * slice_units:(part + 1) * slice_units], down_matrix[part * slice_units:(part + 1) * slice_units], preferred_element_type=jnp.float32))
    return (middle.astype(jnp.float32) + down).astype(jnp.bfloat16)
```

```python
import jax
import jax.numpy as jnp
from jax import lax
from jax.experimental import pallas as pl
from jax.experimental.pallas import tpu as pltpu
from jax.sharding import PartitionSpec as P


HIGH = lax.Precision.HIGHEST
head_eps = 1e-05
row_eps = 1e-06
BF = jnp.bfloat16
F32 = jnp.float32
MESH = pl.DeviceIdType.MESH
LANE = 128


def ring_order(n):
    ys = 1
    while ys * ys * 4 <= n:
        ys *= 2
    zs = n // ys
    if ys * zs != n or ys < 2 or zs % 2:
        return list(range(n))
    walk = []
    for z in range(zs):
        row = list(range(1, ys))
        walk += [z * ys + y for y in (row if z % 2 == 0 else row[::-1])]
    return walk + [z * ys for z in reversed(range(zs))]


def causal_conv(series, prior, taps):
    width, length = taps.shape[0], series.shape[0]
    padded = jnp.concatenate([prior, series], axis=0).astype(F32)
    total = jnp.zeros(series.shape, F32)
    for offset in range(width):
        total = total + taps[offset].astype(F32)[None, :] * padded[offset : offset + length]
    return jax.nn.silu(total)


def local_heads(conv_values, step, within, keys, reads):
    length, width = conv_values.shape
    heads = step.shape[1]
    size = width // heads
    driven = conv_values.reshape(length, heads, size) * step[:, :, None]
    scores = lax.dot_general(reads, keys, (((1,), (1,)), ((), ())), preferred_element_type=F32)
    mask = jnp.tril(jnp.ones((length, length), dtype=bool))
    outs, finals = [], []
    for h in range(heads):
        own = within[:, h]
        spread = jnp.where(mask, own[:, None] - own[None, :], 0.0)
        mixing = jnp.where(mask, jnp.exp(spread) * scores, 0.0).astype(BF)
        value = driven[:, h]
        outs.append(jnp.dot(mixing, value.astype(BF), preferred_element_type=F32))
        late = (value * jnp.exp(own[-1] - own)[:, None]).astype(BF)
        finals.append(
            lax.dot_general(late, keys, (((0,), (0,)), ((), ())), preferred_element_type=F32)
        )
    return outs, jnp.concatenate(finals, axis=0)


def finish_heads(outs, incoming, within, reads, gate_inputs, gains):
    size = outs[0].shape[1]
    done = []
    carried = lax.dot_general(
        reads, incoming.astype(BF), (((1,), (1,)), ((), ())), preferred_element_type=F32
    )
    for h, local in enumerate(outs):
        cols = slice(h * size, (h + 1) * size)
        scan_out = local + carried[:, cols] * jnp.exp(within[:, h])[:, None]
        gated = scan_out * jax.nn.silu(gate_inputs[:, cols].astype(F32))
        scale = lax.rsqrt(jnp.mean(gated * gated, axis=-1, keepdims=True) + head_eps)
        done.append((gated * scale * gains[cols][None, :]).astype(BF))
    return jnp.concatenate(done, axis=1)


def row_norm(rows, gain):
    wide = rows.astype(F32)
    scale = lax.rsqrt(jnp.mean(wide * wide, axis=-1, keepdims=True) + row_eps)
    return (wide * scale * gain[None, :]).astype(BF)


def ring_gather(own):
    n = lax.axis_size("sp")
    order = ring_order(n)
    place = [order.index(i) for i in range(n)]
    me = lax.axis_index("sp")
    at = jnp.asarray(place, jnp.int32)[me]
    owners = jnp.asarray(order, jnp.int32)
    ahead = [(order[i], order[(i + 1) % n]) for i in range(n)]
    back = [(b, a) for a, b in ahead]
    rows = own.shape[0]
    whole = jnp.zeros((n * rows,) + own.shape[1:], own.dtype)
    whole = lax.dynamic_update_slice(whole, own, (me * rows, 0))
    up = down = own
    half = n // 2
    for k in range(1, half + 1):
        from_up = owners[(at - k) % n] * rows
        from_down = owners[(at + k) % n] * rows
        if 2 * k == n:
            cut = rows // 2
            up, down = up[:cut], down[cut:]
            from_down = from_down + cut
        up = lax.ppermute(up, "sp", ahead)
        down = lax.ppermute(down, "sp", back)
        whole = lax.dynamic_update_slice(whole, up, (from_up, 0))
        whole = lax.dynamic_update_slice(whole, down, (from_down, 0))
    return whole


def on_device(
    residual,
    small_value_inputs,
    large_value_inputs,
    small_gate_inputs,
    large_gate_inputs,
    state_projections,
    small_step_inputs,
    large_step_inputs,
    small_decay_offsets,
    large_decay_offsets,
    small_decay_rates,
    large_decay_rates,
    small_filter_taps,
    large_filter_taps,
    state_filter_taps,
    small_head_gains,
    large_head_gains,
    small_output_projection,
    large_output_projection,
    channel_norm_gain,
    gate_matrix,
    up_matrix,
    down_matrix,
):
    n = lax.axis_size("sp")
    me = lax.axis_index("sp")
    margin = state_filter_taps.shape[0] - 1
    length, w1 = small_value_inputs.shape
    w2 = large_value_inputs.shape[1]
    state = state_projections.shape[2]
    planes = state_projections.shape[1] * state
    units = gate_matrix.shape[1]
    flat = state_projections.reshape(length, planes)
    series = jnp.concatenate([small_value_inputs, large_value_inputs, flat], axis=1)
    prior = lax.ppermute(
        series[length - margin :], "sp", [(i, i + 1) for i in range(n - 1)]
    )
    pack = jnp.concatenate([gate_matrix, up_matrix, down_matrix.T], axis=1)
    pack, prior = lax.optimization_barrier((pack, prior))
    whole = ring_gather(pack)

    taps = jnp.concatenate(
        [small_filter_taps, large_filter_taps, state_filter_taps.reshape(margin + 1, planes)], axis=1
    )
    conv = causal_conv(series, prior, taps)
    maps = conv[:, w1 + w2 :].astype(BF)
    keys1, reads1, keys2, reads2 = (maps[:, i * state : (i + 1) * state] for i in range(4))

    heads1 = small_decay_rates.shape[0]
    step = jax.nn.softplus(
        jnp.concatenate([small_step_inputs, large_step_inputs], axis=1).astype(F32)
    )
    rates = jnp.concatenate([small_decay_rates, large_decay_rates])
    offsets = jnp.concatenate([small_decay_offsets, large_decay_offsets], axis=1)
    log_decay = -jnp.exp(rates)[None, :] * step + offsets
    lower = jnp.tril(jnp.ones((length, length), F32))
    within = jnp.dot(lower, log_decay, precision=HIGH)

    outs1, final1 = local_heads(conv[:, :w1], step[:, :heads1], within[:, :heads1], keys1, reads1)
    outs2, final2 = local_heads(
        conv[:, w1 : w1 + w2], step[:, heads1:], within[:, heads1:], keys2, reads2
    )
    heads = rates.shape[0]
    total = jnp.exp(within[-1])
    row = jnp.pad(total[None, :], ((0, 15), (0, state - heads)))
    sent = jnp.concatenate([final1, final2, row], axis=0).astype(BF)
    gathered = lax.all_gather(sent, "sp").astype(F32)
    states1 = gathered[:, :w1].reshape(n, heads1, w1 // heads1, state)
    states2 = gathered[:, w1 : w1 + w2].reshape(n, heads - heads1, w2 // (heads - heads1), state)
    totals = gathered[:, w1 + w2, :heads]
    carry1, carry2 = jnp.zeros_like(states1[0]), jnp.zeros_like(states2[0])
    for hop in range(n - 1):
        factor1 = totals[hop, :heads1][:, None, None]
        factor2 = totals[hop, heads1:][:, None, None]
        carry1 = jnp.where(hop < me, carry1 * factor1 + states1[hop], carry1)
        carry2 = jnp.where(hop < me, carry2 * factor2 + states2[hop], carry2)
    carry1, carry2 = carry1.reshape(w1, state), carry2.reshape(w2, state)

    heads_small = finish_heads(
        outs1, carry1, within[:, :heads1], reads1, small_gate_inputs, small_head_gains
    )
    heads_large = finish_heads(
        outs2, carry2, within[:, heads1:], reads2, large_gate_inputs, large_head_gains
    )
    mixed = (
        jnp.dot(heads_small, small_output_projection, preferred_element_type=F32)
        + jnp.dot(heads_large, large_output_projection, preferred_element_type=F32)
    ).astype(BF)
    mixed = lax.psum_scatter(
        mixed,
        "tp",
        scatter_dimension=0,
        tiled=True,
    ).astype(F32)
    middle = (residual.astype(F32) + mixed).astype(BF)
    normed = row_norm(middle, channel_norm_gain)
    normed_all = lax.all_gather(normed, "tp", axis=0, tiled=True)
    gate = jnp.dot(normed_all, whole[:, :units], preferred_element_type=F32)
    up = jnp.dot(normed_all, whole[:, units : 2 * units], preferred_element_type=F32)
    hidden = (jax.nn.silu(gate) * up).astype(BF)
    partial = lax.dot_general(
        hidden, whole[:, 2 * units :], (((1,), (1,)), ((), ())), preferred_element_type=F32
    )
    down = lax.psum_scatter(
        partial.astype(BF), "tp", scatter_dimension=0, tiled=True
    ).astype(F32)
    return (middle.astype(F32) + down).astype(BF)


def geometry(n):
    ys = 1
    while ys * ys * 4 <= n:
        ys *= 2
    return ys, n // ys


def paired(n, tp, units):
    ys, zs = geometry(n)
    return ys == 2 and zs == 4 and tp == 4 and units % LANE == 0


def fused_kernel(
    vs,
    vl,
    gs,
    gl,
    flat,
    steps_s,
    steps_l,
    offs_s,
    offs_l,
    rates_s,
    rates_l,
    taps_s,
    taps_l,
    taps_m,
    gain_s,
    gain_l,
    proj_s,
    proj_l,
    resid,
    cgain,
    gate_m,
    up_m,
    down_m,
    out,
    xbuf,
    gbuf,
    pbuf,
    rbuf,
    hrow,
    srow,
    wrow,
    wcol,
    maps,
    drv,
    late,
    run,
    smsg,
    rmsg,
    loc,
    hbuf,
    part,
    d2d,
    xsend,
    xrecv,
    mid,
    nall,
    hid,
    wg,
    wu,
    wd,
    psum,
    dcol,
    s1,
    k1,
    r1,
    s2,
    k2,
    r2,
    lsem,
    hs_sem,
    hr_sem,
    ws_sem,
    wy_sem,
    wr_sem,
    wl_sem,
    ms_sem,
    mr_sem,
    ds_sem,
    dr_sem,
    xs_sem,
    xr_sem,
    as_sem,
    ar_sem,
    p_sem,
    q_sem,
    f1s_sem,
    f1r_sem,
    f2s_sem,
    f2r_sem,
):
    n = lax.axis_size("sp")
    sp, tp = lax.axis_index("sp"), lax.axis_index("tp")
    z, y = sp // 2, sp % 2
    pair, zz = z // 2, z % 2
    x, c = tp // 2, tp % 2
    length, w1 = vs.shape
    w2 = vl.shape[1]
    width = w1 + w2
    planes = flat.shape[1]
    state = planes // 4
    heads1, heads2 = steps_s.shape[0], steps_l.shape[0]
    halo = xbuf.shape[0] - length
    rows, units = gate_m.shape
    cols = down_m.shape[1]
    half = wg.shape[1]
    lift = units - half
    own = resid.shape[0]
    tokens = nall.shape[0]
    model = nall.shape[1]
    inner = jnp.where(pair != zz, 1, 0) == 1
    dz = 1 - 2 * pair

    def at(zi, yi):
        return (zi * 2 + yi, tp)

    mate_z = at(z + 1 - 2 * zz, y)
    mate_y = at(z, 1 - y)
    mate_x = (sp, (1 - x) * 2 + c)
    mate_c = (sp, x * 2 + 1 - c)

    def remote(src, dst, send, recv, device):
        return pltpu.make_async_remote_copy(
            src_ref=src, dst_ref=dst, send_sem=send, recv_sem=recv, device_id=device, device_id_type=MESH
        )

    barrier = pltpu.get_barrier_semaphore()
    peers = [(lax.rem(sp + k, n), tp) for k in range(1, n)] + [mate_x, mate_c]
    for peer in peers:
        pl.semaphore_signal(barrier, inc=1, device_id=peer, device_id_type=MESH)
    loads = []
    for src, dst in (
        (vs, xbuf.at[pl.ds(halo, length), pl.ds(0, w1)]),
        (vl, xbuf.at[pl.ds(halo, length), pl.ds(w1, w2)]),
        (flat, xbuf.at[pl.ds(halo, length), pl.ds(width, planes)]),
        (gs, gbuf.at[:, pl.ds(0, w1)]),
        (gl, gbuf.at[:, pl.ds(w1, w2)]),
        (proj_s, pbuf.at[pl.ds(0, w1), :]),
        (proj_l, pbuf.at[pl.ds(w1, w2), :]),
        (resid, rbuf),
    ):
        copy = pltpu.make_async_copy(src, dst, lsem.at[len(loads)])
        copy.start()
        loads.append(copy)
    pl.semaphore_wait(barrier, len(peers))

    halos = []
    for i, (src, lo, size) in enumerate(((vs, 0, w1), (vl, w1, w2), (flat, width, planes))):
        halos.append(
            remote(
                src.at[pl.ds(length - halo, halo), :],
                xbuf.at[pl.ds(0, halo), pl.ds(lo, size)],
                hs_sem.at[i],
                hr_sem.at[i],
                (lax.rem(sp + 1, n), tp),
            )
        )

    @pl.when(sp < n - 1)
    def _():
        for copy in halos:
            copy.start()

    def source(p, h):
        cut = pl.ds(pl.multiple_of(h * lift, LANE), half)
        return (gate_m.at[:, cut], up_m.at[:, cut], down_m.at[cut, :])[p]

    def place(p, b):
        if p == 2:
            return wd.at[b]
        return (wg, wu)[p].at[pl.ds(pl.multiple_of(b * rows, rows), rows), :]

    def weight_wait(p, b):
        remote(place(p, b), place(p, b), ws_sem.at[0, 0], wr_sem.at[p, b], mate_y).wait_recv()

    keep = [pltpu.make_async_copy(source(p, zz), place(p, sp), wl_sem.at[p]) for p in range(3)]
    other = [
        remote(source(p, 1 - zz), place(p, sp), ws_sem.at[0, p], wr_sem.at[p, sp], at(z + dz, y)) for p in range(3)
    ]
    same = [
        remote(source(p, zz), place(p, sp), ws_sem.at[1, p], wr_sem.at[p, sp], at(z + 2 * dz, y)) for p in range(3)
    ]
    outer_z = jnp.clip(z - dz, 0, 3)
    back = [
        remote(source(p, 1 - zz), place(p, sp), ws_sem.at[2, p], wr_sem.at[p, sp], at(outer_z, y)) for p in range(3)
    ]
    near = (2 * pair + 1 - zz) * 2 + y
    relay = [
        remote(place(p, near), place(p, near), ws_sem.at[3, p], wr_sem.at[p, near], at(z + 2 * dz, y))
        for p in range(3)
    ]
    across = [
        remote(source(p, zz), place(p, sp), wy_sem.at[0, p], wr_sem.at[p, sp], mate_y) for p in range(3)
    ]
    line = [near, (2 - pair) * 2 + y, (3 - 3 * pair) * 2 + y]
    spread = [
        [
            remote(place(p, b), place(p, b), wy_sem.at[1 + j, p], wr_sem.at[p, b], mate_y)
            for p in range(3)
        ]
        for j, b in enumerate(line)
    ]

    def first_sends(p):
        other[p].start()

        @pl.when(inner)
        def _():
            back[p].start()

        across[p].start()

    def service(j, p):
        weight_wait(p, line[j])
        spread[j][p].start()
        if j == 0:

            @pl.when(inner)
            def _():
                relay[p].start()

    first_sends(0)
    for copy in keep:
        copy.start()

    hrow[...] = jnp.zeros_like(hrow)
    srow[...] = jnp.zeros_like(srow)
    raw_s = steps_s[...].astype(F32)
    raw_l = steps_l[...].astype(F32)
    srow[0:heads1, :] = jnp.maximum(raw_s, 0.0) + jnp.log1p(jnp.exp(-jnp.abs(raw_s)))
    srow[heads1 : heads1 + heads2, :] = jnp.maximum(raw_l, 0.0) + jnp.log1p(jnp.exp(-jnp.abs(raw_l)))
    for h in range(heads1 + heads2):
        rate = rates_s[h] if h < heads1 else rates_l[h - heads1]
        offset = offs_s[h : h + 1, :] if h < heads1 else offs_l[h - heads1 : h - heads1 + 1, :]
        hrow[h : h + 1, :] = offset - jnp.exp(jnp.full((1, length), rate, F32)) * srow[h : h + 1, :]
    chunks = length // LANE
    ri = lax.broadcasted_iota(jnp.int32, (LANE, LANE), 0)
    ci = lax.broadcasted_iota(jnp.int32, (LANE, LANE), 1)
    upper = jnp.where(ri <= ci, 1.0, 0.0).astype(F32)
    slab = hrow.shape[0]
    stacked = jnp.concatenate([hrow[:, k * LANE : (k + 1) * LANE] for k in range(chunks)], axis=0)
    sums = lax.dot_general(
        stacked, upper, (((1,), (0,)), ((), ())), precision=HIGH, preferred_element_type=F32
    )
    base = jnp.zeros((slab, 1), F32)
    fill = jnp.zeros((LANE - 2 * slab, LANE), F32)
    for k in range(chunks):
        w = sums[k * slab : (k + 1) * slab] + base
        base = w[:, LANE - 1 : LANE]
        cut = slice(k * LANE, (k + 1) * LANE)
        wrow[:, cut] = w
        wcol[cut, :] = jnp.concatenate([w, srow[:, cut], fill], axis=0).T

    for copy in loads[:3]:
        copy.wait()

    @pl.when(sp > 0)
    def _():
        for copy in halos:
            copy.wait_recv()

    @pl.when(sp == 0)
    def _():
        xbuf[0:halo, :] = jnp.zeros((halo, width + planes), BF)

    def conv(lo, taps):
        wide = xbuf[:, lo : lo + LANE].astype(F32)
        total = wide * taps[-1]
        for k in range(len(taps) - 1):
            total = total + taps[k] * pltpu.roll(wide, len(taps) - 1 - k, 0)
        total = total[halo:]
        return total * jax.nn.sigmoid(total)

    count = taps_s.shape[0]
    for i in range(4):
        taps = [taps_m[k, i : i + 1, :].astype(F32) for k in range(count)]
        maps[:, i * LANE : (i + 1) * LANE] = conv(width + i * LANE, taps).astype(BF)
    lane = lax.broadcasted_iota(jnp.int32, (1, LANE), 1)
    size1, size2 = w1 // heads1, w2 // heads2

    def tile_heads(j):
        if j * LANE < w1:
            return [j * LANE // size1 + i for i in range(LANE // size1)], size1
        return [heads1 + (j * LANE - w1) // size2], size2

    def by_head(values, size):
        total = values[-1]
        for i in reversed(range(len(values) - 1)):
            total = jnp.where(lane < (i + 1) * size, values[i], total)
        return total

    def spread_cols(j, offset):
        own_heads, size = tile_heads(j)
        return by_head(
            [jnp.broadcast_to(wcol[:, offset + h : offset + h + 1], (length, LANE)) for h in own_heads], size
        )

    tiles = width // LANE
    slot = 0
    slots = {}
    for j in range(tiles):
        lo = j * LANE
        ref, at_lo = (taps_s, lo) if lo < w1 else (taps_l, lo - w1)
        taps = [ref[k : k + 1, at_lo : at_lo + LANE].astype(F32) for k in range(count)]
        driven = conv(lo, taps) * spread_cols(j, slab)
        own_heads, size = tile_heads(j)
        last = by_head([jnp.broadcast_to(wrow[h : h + 1, length - 1 : length], (1, LANE)) for h in own_heads], size)
        within = spread_cols(j, 0)
        late[:, lo : lo + LANE] = (driven * jnp.exp(last - within)).astype(BF)
        run[state : state + 1, lo : lo + LANE] = jnp.exp(last)
        for i, h in enumerate(own_heads):
            keep_lanes = driven
            if len(own_heads) > 1:
                keep_lanes = jnp.where((lane >= i * size) & (lane < (i + 1) * size), driven, 0.0)
            drv[:, slot * LANE : (slot + 1) * LANE] = keep_lanes.astype(BF)
            slots[h] = slot
            slot += 1

    for kind, lo, size in ((0, 0, w1), (1, w1, w2)):
        keys = maps[:, 2 * kind * LANE : (2 * kind + 1) * LANE]
        run[0:state, lo : lo + size] = lax.dot_general(
            keys, late[:, lo : lo + size], (((0,), (0,)), ((), ())), preferred_element_type=F32
        )
    run[state + 8 : 2 * state + 8, :] = jnp.zeros((state, width), F32)
    run[2 * state + 8 : 2 * state + 9, :] = jnp.ones((1, width), F32)
    messages = []
    while (1 << len(messages)) < n:
        k = len(messages)
        messages.append(
            remote(smsg.at[k], rmsg.at[k], ms_sem.at[k], mr_sem.at[k], (lax.rem(sp + (1 << k), n), tp))
        )

    def send_state(k):
        smsg[k, 0:state, :] = run[0:state, :].astype(BF)
        smsg[k, state : state + 16, :] = jnp.broadcast_to(run[state : state + 1, :], (16, width)).astype(BF)

        @pl.when(sp + (1 << k) < n)
        def _():
            messages[k].start()

    def take_state(k):
        @pl.when(sp >= (1 << k))
        def _():
            messages[k].wait_recv()
            got = rmsg[k, 0:state, :].astype(F32)
            decay = rmsg[k, state : state + 1, :].astype(F32)
            a, b = state + 8, 2 * state + 8
            before = run[b : b + 1, :]
            run[a:b, :] = got * before + run[a:b, :]
            run[b : b + 1, :] = decay * before
            if k + 1 < len(messages):
                here = run[state : state + 1, :]
                run[0:state, :] = got * here + run[0:state, :]
                run[state : state + 1, :] = decay * here

    kinds = [[h for h in slots if h < heads1], [h for h in slots if h >= heads1]]

    def local_rows(i):
        r0 = i * LANE
        size_k = r0 + LANE
        rowid = lax.broadcasted_iota(jnp.int32, (LANE, size_k), 0) + r0
        colid = lax.broadcasted_iota(jnp.int32, (LANE, size_k), 1)
        mask = colid <= rowid
        for kind in range(2):
            keys = maps[0:size_k, 2 * kind * LANE : (2 * kind + 1) * LANE]
            reads = maps[r0 : r0 + LANE, (2 * kind + 1) * LANE : (2 * kind + 2) * LANE]
            scores = lax.dot_general(reads, keys, (((1,), (1,)), ((), ())), preferred_element_type=F32)
            for j in range(tiles):
                own_heads, _ = tile_heads(j)
                if own_heads[0] not in kinds[kind]:
                    continue
                total = None
                for h in own_heads:
                    spread_h = wcol[r0 : r0 + LANE, h : h + 1] - wrow[h : h + 1, 0:size_k]
                    mixing = (jnp.exp(jnp.where(mask, spread_h, -1e30)) * scores).astype(BF)
                    term = jnp.dot(
                        mixing,
                        drv[0:size_k, slots[h] * LANE : (slots[h] + 1) * LANE],
                        preferred_element_type=F32,
                    )
                    total = term if total is None else total + term
                loc[r0 : r0 + LANE, j * LANE : (j + 1) * LANE] = total

    send_state(0)
    first_sends(1)
    cuts = [chunks * k // len(messages) for k in range(len(messages) + 1)]
    for k in range(len(messages)):
        for i in range(cuts[k], cuts[k + 1]):
            local_rows(i)
        take_state(k)
        if k + 1 < len(messages):
            send_state(k + 1)
        if k == 0:
            first_sends(2)
        if k == 1:
            for copy in same:
                copy.start()
            service(0, 0)
            service(0, 1)

    for copy in loads[3:]:
        copy.wait()
    for j in range(tiles):
        lo = j * LANE
        kind = 0 if lo < w1 else 1
        own_heads, size = tile_heads(j)
        reads = maps[:, (2 * kind + 1) * LANE : (2 * kind + 2) * LANE]
        carry = run[state + 8 : 2 * state + 8, lo : lo + LANE].astype(BF)
        carried = jnp.dot(reads, carry, preferred_element_type=F32)
        scan_out = loc[:, lo : lo + LANE] + carried * jnp.exp(spread_cols(j, 0))
        gates = gbuf[:, lo : lo + LANE].astype(F32)
        gated = scan_out * (gates * jax.nn.sigmoid(gates))
        square = gated * gated
        scales = []
        for i in range(len(own_heads)):
            one = square
            if len(own_heads) > 1:
                one = jnp.where((lane >= i * size) & (lane < (i + 1) * size), square, 0.0)
            mean = jnp.sum(one, axis=1, keepdims=True) * (1.0 / size)
            scales.append(jnp.broadcast_to(lax.rsqrt(mean + head_eps), (length, LANE)))
        ref, at_lo = (gain_s, lo) if lo < w1 else (gain_l, lo - w1)
        gain = ref[0:1, at_lo : at_lo + LANE]
        hbuf[:, lo : lo + LANE] = (gated * by_head(scales, size) * gain).astype(BF)

    wide = 2 * LANE

    @pl.loop(0, model // wide)
    def _(i):
        cut = pl.ds(pl.multiple_of(i * wide, wide), wide)
        part[:, cut] = jnp.dot(hbuf[...], pbuf[:, cut], preferred_element_type=F32).astype(BF)

    def rows_of(xi, ci):
        return pl.ds(pl.multiple_of((xi * 2 + ci) * own, own), own)

    cores = [
        remote(part.at[rows_of(xi, 1 - c), :], d2d.at[i], ds_sem.at[i], dr_sem.at[i], mate_c)
        for i, xi in enumerate((1 - x, x))
    ]
    for copy in cores:
        copy.start()
    service(0, 2)
    cores[0].wait_recv()
    xsend[...] = (part[rows_of(1 - x, c), :].astype(F32) + d2d[0].astype(F32)).astype(BF)
    cross = remote(xsend, xrecv, xs_sem.at[0], xr_sem.at[0], mate_x)
    cross.start()
    for p in range(3):
        service(1, p)
    cores[1].wait_recv()
    cross.wait_recv()
    mixed = part[rows_of(x, c), :].astype(F32) + d2d[1].astype(F32) + xrecv[...].astype(F32)
    middle = (rbuf[...].astype(F32) + mixed).astype(BF)
    mid[...] = middle
    broad = middle.astype(F32)
    scale = lax.rsqrt(jnp.mean(broad * broad, axis=-1, keepdims=True) + row_eps)

    def place_rows(zi, xi, ci):
        index = zi * 4 + ci * 2 + xi
        return index, nall.at[pl.ds(pl.multiple_of(index * own, own), own), :]

    _, my_rows = place_rows(zz, x, c)
    my_rows[...] = (broad * scale * cgain[...]).astype(BF)

    def share(i, zi, xi, ci, device):
        index, view = place_rows(zi, xi, ci)
        return remote(view, view, as_sem.at[i], ar_sem.at[index], device)

    def rows_wait(zi, xi, ci):
        share(0, zi, xi, ci, mate_c).wait_recv()

    shares = [
        share(0, zz, x, c, mate_x),
        share(1, zz, x, c, mate_z),
        share(2, zz, x, c, mate_c),
        share(3, zz, 1 - x, c, mate_c),
        share(4, 1 - zz, x, c, mate_x),
        share(5, 1 - zz, x, c, mate_c),
        share(6, 1 - zz, 1 - x, c, mate_c),
    ]
    for i in range(3):
        shares[i].start()
    rows_wait(zz, 1 - x, c)
    shares[3].start()
    rows_wait(1 - zz, x, c)
    shares[4].start()
    shares[5].start()

    for copy in keep:
        copy.wait()
    for p in range(2):
        service(2, p)

    far = [k * 2 + 1 - y for k in range(4)]
    for p in range(2):
        for b in far:
            weight_wait(p, b)
    rows_wait(zz, x, 1 - c)
    rows_wait(zz, 1 - x, 1 - c)
    hot = wide if half % wide == 0 else LANE
    first = zz * (2 * half - units)

    def up_rows(zi):
        span = pl.ds(pl.multiple_of(zi * (tokens // 2), tokens // 2), tokens // 2)

        @pl.loop(0, half // hot)
        def _(i):
            cut = pl.ds(pl.multiple_of(i * hot, hot), hot)
            have = nall[span, :]
            gate = jnp.dot(have, wg[:, cut], preferred_element_type=F32)
            up = jnp.dot(have, wu[:, cut], preferred_element_type=F32)
            unit = lax.broadcasted_iota(jnp.int32, (1, hot), 1) + i * hot
            value = gate * jax.nn.sigmoid(gate) * up
            hid[span, cut] = jnp.where(unit >= first, value, 0.0).astype(BF)

    up_rows(zz)
    rows_wait(1 - zz, 1 - x, c)
    shares[6].start()
    rows_wait(1 - zz, x, 1 - c)
    rows_wait(1 - zz, 1 - x, 1 - c)
    up_rows(1 - zz)
    service(2, 2)

    order = [
        ((2 * jnp.bitwise_xor(pair, dp) + k) * 2 + jnp.bitwise_xor(y, dy)) for dp in (0, 1) for dy in (0, 1) for k in (0, 1)
    ]
    known = [dy == 0 for _ in range(2) for dy in (0, 1) for _ in range(2)]
    core_rows = tokens // 4

    def strip(zi, ci):
        return pl.ds(pl.multiple_of(zi * (tokens // 2) + ci * core_rows, core_rows), core_rows)

    def swap(q):
        return [
            remote(
                psum.at[q, strip(zi, 1 - c), :],
                dcol.at[q, pl.ds(zi * core_rows, core_rows), :],
                p_sem.at[q, zi],
                q_sem.at[q, zi],
                mate_c,
            )
            for zi in range(2)
        ]

    def hop1(q):
        return remote(s1.at[q], r1.at[q], f1s_sem.at[q], f1r_sem.at[q], mate_z if q % 2 == 0 else mate_x)

    def hop2(q):
        return remote(s2.at[q], r2.at[q], f2s_sem.at[q], f2r_sem.at[q], mate_x if q % 2 == 0 else mate_z)

    def compute(q):
        if not known[q]:
            weight_wait(2, order[q])

        @pl.loop(0, 4)
        def _(i):
            span = pl.ds(pl.multiple_of(i * core_rows, core_rows), core_rows)
            psum[q, span, :] = jnp.dot(
                hid[span, :], wd[order[q]], preferred_element_type=F32
            ).astype(BF)

        for copy in swap(q):
            copy.start()

    def sum1(q):
        for copy in swap(q):
            copy.wait_recv()
        for j in range(2):
            for send in (True, False):
                if q % 2 == 0:
                    zi, xi = (1 - zz if send else zz), j
                else:
                    zi, xi = j, (1 - x if send else x)
                a = pl.ds(pl.multiple_of(zi * (tokens // 2) + c * core_rows + xi * own, own), own)
                b = pl.ds(pl.multiple_of(zi * core_rows + xi * own, own), own)
                total = psum[q, a, :].astype(F32) + dcol[q, b, :].astype(F32)
                to = slice(j * own, (j + 1) * own)
                if send:
                    s1[q, to, :] = total.astype(BF)
                else:
                    k1[q, to, :] = total
        hop1(q).start()

    def sum2(q):
        hop1(q).wait_recv()
        second = x if q % 2 == 0 else zz
        for send in (True, False):
            j = 1 - second if send else second
            cut = pl.ds(pl.multiple_of(j * own, own), own)
            total = k1[q, cut, :] + r1[q, cut, :].astype(F32)
            if send:
                s2[q] = total.astype(BF)
            else:
                k2[q] = total
        hop2(q).start()

    def sum3(q):
        hop2(q).wait_recv()
        cut = pl.ds(pl.multiple_of(order[q] * cols, cols), cols)
        out[:, cut] = (mid[:, cut].astype(F32) + k2[q] + r2[q].astype(F32)).astype(BF)

    stages = (compute, sum1, sum2, sum3)
    for step in range(n + len(stages) - 1):
        for i, stage in enumerate(stages):
            if 0 <= step - i < n:
                stage(step - i)

    @pl.when(sp < n - 1)
    def _():
        for copy in halos:
            copy.wait_send()

    for k, copy in enumerate(messages):

        @pl.when(sp + (1 << k) < n)
        def _(copy=copy):
            copy.wait_send()

    for p in range(3):
        other[p].wait_send()
        same[p].wait_send()
        across[p].wait_send()
        for j in range(3):
            spread[j][p].wait_send()

        @pl.when(inner)
        def _(p=p):
            back[p].wait_send()
            relay[p].wait_send()

    for copy in cores + [cross] + shares:
        copy.wait_send()
    for q in range(n):
        for copy in swap(q) + [hop1(q), hop2(q)]:
            copy.wait_send()


def fused_layer(
    residual,
    small_value_inputs,
    large_value_inputs,
    small_gate_inputs,
    large_gate_inputs,
    state_projections,
    small_step_inputs,
    large_step_inputs,
    small_decay_offsets,
    large_decay_offsets,
    small_decay_rates,
    large_decay_rates,
    small_filter_taps,
    large_filter_taps,
    state_filter_taps,
    small_head_gains,
    large_head_gains,
    small_output_projection,
    large_output_projection,
    channel_norm_gain,
    gate_matrix,
    up_matrix,
    down_matrix,
):
    n = lax.axis_size("sp")
    length, w1 = small_value_inputs.shape
    w2 = large_value_inputs.shape[1]
    width = w1 + w2
    state = state_projections.shape[2]
    planes = state_projections.shape[1] * state
    heads = small_decay_rates.shape[0] + large_decay_rates.shape[0]
    rows, units = gate_matrix.shape
    cols = down_matrix.shape[1]
    own, model = residual.shape
    tiles = units // LANE
    half = (tiles + 1) // 2 * LANE
    halo = 16
    slab = 8 * ((heads + 7) // 8)
    tokens = 2 * length
    hops = max(1, (n - 1).bit_length())
    vmem, dma = pltpu.VMEM, pltpu.SemaphoreType.DMA
    hbm = pl.BlockSpec(memory_space=pl.ANY)
    near = pl.BlockSpec(memory_space=pltpu.VMEM)
    scalar = pl.BlockSpec(memory_space=pltpu.SMEM)
    specs = [hbm] * 5 + [near] * 4 + [scalar] * 2 + [near] * 5 + [hbm] * 3 + [near] + [hbm] * 3
    scratch = [
        vmem((length + halo, width + planes), BF),
        vmem((length, width), BF),
        vmem((width, model), BF),
        vmem((own, model), BF),
        vmem((slab, length), F32),
        vmem((slab, length), F32),
        vmem((slab, length), F32),
        vmem((length, LANE), F32),
        vmem((length, planes), BF),
        vmem((length, heads * LANE), BF),
        vmem((length, width), BF),
        vmem((2 * state + 16, width), F32),
        vmem((hops, state + 16, width), BF),
        vmem((hops, state + 16, width), BF),
        vmem((length, width), F32),
        vmem((length, width), BF),
        vmem((length, model), BF),
        vmem((2, own, model), BF),
        vmem((own, model), BF),
        vmem((own, model), BF),
        vmem((own, model), BF),
        vmem((tokens, model), BF),
        vmem((tokens, half), BF),
        vmem((n * rows, half), BF),
        vmem((n * rows, half), BF),
        vmem((n, half, cols), BF),
        vmem((n, tokens, cols), BF),
        vmem((n, tokens // 2, cols), BF),
        vmem((n, 2 * own, cols), BF),
        vmem((n, 2 * own, cols), F32),
        vmem((n, 2 * own, cols), BF),
        vmem((n, own, cols), BF),
        vmem((n, own, cols), F32),
        vmem((n, own, cols), BF),
        dma((8,)),
        dma((3,)),
        dma((3,)),
        dma((4, 3)),
        dma((4, 3)),
        dma((3, n)),
        dma((3,)),
        dma((hops,)),
        dma((hops,)),
        dma((2,)),
        dma((2,)),
        dma((1,)),
        dma((1,)),
        dma((7,)),
        dma((8,)),
        dma((n, 2)),
        dma((n, 2)),
        dma((n,)),
        dma((n,)),
        dma((n,)),
        dma((n,)),
    ]
    return pl.pallas_call(
        fused_kernel,
        out_shape=jax.ShapeDtypeStruct((own, model), BF),
        in_specs=specs,
        out_specs=pl.BlockSpec(memory_space=pltpu.VMEM),
        scratch_shapes=scratch,
        compiler_params=pltpu.CompilerParams(
            collective_id=0, has_side_effects=True, vmem_limit_bytes=66 * 1024 * 1000
        ),
    )(
        small_value_inputs,
        large_value_inputs,
        small_gate_inputs,
        large_gate_inputs,
        state_projections.reshape(length, planes),
        small_step_inputs.T,
        large_step_inputs.T,
        small_decay_offsets.T,
        large_decay_offsets.T,
        small_decay_rates,
        large_decay_rates,
        small_filter_taps,
        large_filter_taps,
        state_filter_taps,
        small_head_gains.reshape(1, w1),
        large_head_gains.reshape(1, w2),
        small_output_projection,
        large_output_projection,
        residual,
        channel_norm_gain.reshape(1, model),
        gate_matrix,
        up_matrix,
        down_matrix,
    )


def solution(mesh):
    in_specs = (
        P(("sp", "tp"), None),
        P("sp", "tp"),
        P("sp", "tp"),
        P("sp", "tp"),
        P("sp", "tp"),
        P("sp", None, None),
        P("sp", "tp"),
        P("sp", "tp"),
        P("sp", "tp"),
        P("sp", "tp"),
        P("tp"),
        P("tp"),
        P(None, "tp"),
        P(None, "tp"),
        P(),
        P("tp"),
        P("tp"),
        P("tp", None),
        P("tp", None),
        P(),
        P("sp", "tp"),
        P("sp", "tp"),
        P("tp", "sp"),
    )

    def layer(*args):
        units = args[20].shape[1]
        if paired(mesh.shape["sp"], mesh.shape["tp"], units):
            return fused_layer(*args)
        return on_device(*args)

    return jax.shard_map(
        layer,
        mesh=mesh,
        in_specs=in_specs,
        out_specs=P(("sp", "tp"), None),
        check_vma=False,
    )
```

```python
import jax
import jax.numpy as jnp
from jax import lax
from jax.experimental import pallas as pl
from jax.experimental.pallas import tpu as pltpu
from jax.sharding import PartitionSpec as P


HIGH = lax.Precision.HIGHEST
head_eps = 1e-05
row_eps = 1e-06
BF = jnp.bfloat16
F32 = jnp.float32
MESH = pl.DeviceIdType.MESH
LANE = 128


def ring_order(n):
    ys = 1
    while ys * ys * 4 <= n:
        ys *= 2
    zs = n // ys
    if ys * zs != n or ys < 2 or zs % 2:
        return list(range(n))
    walk = []
    for z in range(zs):
        row = list(range(1, ys))
        walk += [z * ys + y for y in (row if z % 2 == 0 else row[::-1])]
    return walk + [z * ys for z in reversed(range(zs))]


def causal_conv(series, prior, taps):
    width, length = taps.shape[0], series.shape[0]
    padded = jnp.concatenate([prior, series], axis=0).astype(F32)
    total = jnp.zeros(series.shape, F32)
    for offset in range(width):
        total = total + taps[offset].astype(F32)[None, :] * padded[offset : offset + length]
    return jax.nn.silu(total)


def local_heads(conv_values, step, within, keys, reads):
    length, width = conv_values.shape
    heads = step.shape[1]
    size = width // heads
    driven = conv_values.reshape(length, heads, size) * step[:, :, None]
    scores = lax.dot_general(reads, keys, (((1,), (1,)), ((), ())), preferred_element_type=F32)
    mask = jnp.tril(jnp.ones((length, length), dtype=bool))
    outs, finals = [], []
    for h in range(heads):
        own = within[:, h]
        spread = jnp.where(mask, own[:, None] - own[None, :], 0.0)
        mixing = jnp.where(mask, jnp.exp(spread) * scores, 0.0).astype(BF)
        value = driven[:, h]
        outs.append(jnp.dot(mixing, value.astype(BF), preferred_element_type=F32))
        late = (value * jnp.exp(own[-1] - own)[:, None]).astype(BF)
        finals.append(
            lax.dot_general(late, keys, (((0,), (0,)), ((), ())), preferred_element_type=F32)
        )
    return outs, jnp.concatenate(finals, axis=0)


def finish_heads(outs, incoming, within, reads, gate_inputs, gains):
    size = outs[0].shape[1]
    done = []
    carried = lax.dot_general(
        reads, incoming.astype(BF), (((1,), (1,)), ((), ())), preferred_element_type=F32
    )
    for h, local in enumerate(outs):
        cols = slice(h * size, (h + 1) * size)
        scan_out = local + carried[:, cols] * jnp.exp(within[:, h])[:, None]
        gated = scan_out * jax.nn.silu(gate_inputs[:, cols].astype(F32))
        scale = lax.rsqrt(jnp.mean(gated * gated, axis=-1, keepdims=True) + head_eps)
        done.append((gated * scale * gains[cols][None, :]).astype(BF))
    return jnp.concatenate(done, axis=1)


def row_norm(rows, gain):
    wide = rows.astype(F32)
    scale = lax.rsqrt(jnp.mean(wide * wide, axis=-1, keepdims=True) + row_eps)
    return (wide * scale * gain[None, :]).astype(BF)


def ring_gather(own):
    n = lax.axis_size("sp")
    order = ring_order(n)
    place = [order.index(i) for i in range(n)]
    me = lax.axis_index("sp")
    at = jnp.asarray(place, jnp.int32)[me]
    owners = jnp.asarray(order, jnp.int32)
    ahead = [(order[i], order[(i + 1) % n]) for i in range(n)]
    back = [(b, a) for a, b in ahead]
    rows = own.shape[0]
    whole = jnp.zeros((n * rows,) + own.shape[1:], own.dtype)
    whole = lax.dynamic_update_slice(whole, own, (me * rows, 0))
    up = down = own
    half = n // 2
    for k in range(1, half + 1):
        from_up = owners[(at - k) % n] * rows
        from_down = owners[(at + k) % n] * rows
        if 2 * k == n:
            cut = rows // 2
            up, down = up[:cut], down[cut:]
            from_down = from_down + cut
        up = lax.ppermute(up, "sp", ahead)
        down = lax.ppermute(down, "sp", back)
        whole = lax.dynamic_update_slice(whole, up, (from_up, 0))
        whole = lax.dynamic_update_slice(whole, down, (from_down, 0))
    return whole


def on_device(
    residual,
    small_value_inputs,
    large_value_inputs,
    small_gate_inputs,
    large_gate_inputs,
    state_projections,
    small_step_inputs,
    large_step_inputs,
    small_decay_offsets,
    large_decay_offsets,
    small_decay_rates,
    large_decay_rates,
    small_filter_taps,
    large_filter_taps,
    state_filter_taps,
    small_head_gains,
    large_head_gains,
    small_output_projection,
    large_output_projection,
    channel_norm_gain,
    gate_matrix,
    up_matrix,
    down_matrix,
):
    n = lax.axis_size("sp")
    me = lax.axis_index("sp")
    margin = state_filter_taps.shape[0] - 1
    length, w1 = small_value_inputs.shape
    w2 = large_value_inputs.shape[1]
    state = state_projections.shape[2]
    planes = state_projections.shape[1] * state
    units = gate_matrix.shape[1]
    flat = state_projections.reshape(length, planes)
    series = jnp.concatenate([small_value_inputs, large_value_inputs, flat], axis=1)
    prior = lax.ppermute(
        series[length - margin :], "sp", [(i, i + 1) for i in range(n - 1)]
    )
    pack = jnp.concatenate([gate_matrix, up_matrix, down_matrix.T], axis=1)
    pack, prior = lax.optimization_barrier((pack, prior))
    whole = ring_gather(pack)

    taps = jnp.concatenate(
        [small_filter_taps, large_filter_taps, state_filter_taps.reshape(margin + 1, planes)], axis=1
    )
    conv = causal_conv(series, prior, taps)
    maps = conv[:, w1 + w2 :].astype(BF)
    keys1, reads1, keys2, reads2 = (maps[:, i * state : (i + 1) * state] for i in range(4))

    heads1 = small_decay_rates.shape[0]
    step = jax.nn.softplus(
        jnp.concatenate([small_step_inputs, large_step_inputs], axis=1).astype(F32)
    )
    rates = jnp.concatenate([small_decay_rates, large_decay_rates])
    offsets = jnp.concatenate([small_decay_offsets, large_decay_offsets], axis=1)
    log_decay = -jnp.exp(rates)[None, :] * step + offsets
    lower = jnp.tril(jnp.ones((length, length), F32))
    within = jnp.dot(lower, log_decay, precision=HIGH)

    outs1, final1 = local_heads(conv[:, :w1], step[:, :heads1], within[:, :heads1], keys1, reads1)
    outs2, final2 = local_heads(
        conv[:, w1 : w1 + w2], step[:, heads1:], within[:, heads1:], keys2, reads2
    )
    heads = rates.shape[0]
    total = jnp.exp(within[-1])
    row = jnp.pad(total[None, :], ((0, 15), (0, state - heads)))
    sent = jnp.concatenate([final1, final2, row], axis=0).astype(BF)
    gathered = lax.all_gather(sent, "sp").astype(F32)
    states1 = gathered[:, :w1].reshape(n, heads1, w1 // heads1, state)
    states2 = gathered[:, w1 : w1 + w2].reshape(n, heads - heads1, w2 // (heads - heads1), state)
    totals = gathered[:, w1 + w2, :heads]
    carry1, carry2 = jnp.zeros_like(states1[0]), jnp.zeros_like(states2[0])
    for hop in range(n - 1):
        factor1 = totals[hop, :heads1][:, None, None]
        factor2 = totals[hop, heads1:][:, None, None]
        carry1 = jnp.where(hop < me, carry1 * factor1 + states1[hop], carry1)
        carry2 = jnp.where(hop < me, carry2 * factor2 + states2[hop], carry2)
    carry1, carry2 = carry1.reshape(w1, state), carry2.reshape(w2, state)

    heads_small = finish_heads(
        outs1, carry1, within[:, :heads1], reads1, small_gate_inputs, small_head_gains
    )
    heads_large = finish_heads(
        outs2, carry2, within[:, heads1:], reads2, large_gate_inputs, large_head_gains
    )
    mixed = (
        jnp.dot(heads_small, small_output_projection, preferred_element_type=F32)
        + jnp.dot(heads_large, large_output_projection, preferred_element_type=F32)
    ).astype(BF)
    mixed = lax.psum_scatter(
        mixed,
        "tp",
        scatter_dimension=0,
        tiled=True,
    ).astype(F32)
    middle = (residual.astype(F32) + mixed).astype(BF)
    normed = row_norm(middle, channel_norm_gain)
    normed_all = lax.all_gather(normed, "tp", axis=0, tiled=True)
    gate = jnp.dot(normed_all, whole[:, :units], preferred_element_type=F32)
    up = jnp.dot(normed_all, whole[:, units : 2 * units], preferred_element_type=F32)
    hidden = (jax.nn.silu(gate) * up).astype(BF)
    partial = lax.dot_general(
        hidden, whole[:, 2 * units :], (((1,), (1,)), ((), ())), preferred_element_type=F32
    )
    down = lax.psum_scatter(
        partial.astype(BF), "tp", scatter_dimension=0, tiled=True
    ).astype(F32)
    return (middle.astype(F32) + down).astype(BF)


def geometry(n):
    ys = 1
    while ys * ys * 4 <= n:
        ys *= 2
    return ys, n // ys


def paired(n, tp, units):
    ys, zs = geometry(n)
    return ys == 2 and zs == 4 and tp == 4 and units % LANE == 0


def fused_kernel(
    vs,
    vl,
    gs,
    gl,
    flat,
    steps_s,
    steps_l,
    offs_s,
    offs_l,
    rates_s,
    rates_l,
    taps_s,
    taps_l,
    taps_m,
    gain_s,
    gain_l,
    proj_s,
    proj_l,
    resid,
    cgain,
    gate_m,
    up_m,
    down_m,
    out,
    xbuf,
    gbuf,
    pbuf,
    rbuf,
    hrow,
    srow,
    wrow,
    wcol,
    maps,
    drv,
    late,
    run,
    smsg,
    rmsg,
    loc,
    hbuf,
    part,
    d2d,
    xsend,
    xrecv,
    mid,
    nall,
    hid,
    wg,
    wu,
    wd,
    psum,
    dcol,
    s1,
    k1,
    r1,
    s2,
    k2,
    r2,
    lsem,
    hs_sem,
    hr_sem,
    ws_sem,
    wy_sem,
    wr_sem,
    wl_sem,
    ms_sem,
    mr_sem,
    ds_sem,
    dr_sem,
    xs_sem,
    xr_sem,
    as_sem,
    ar_sem,
    p_sem,
    q_sem,
    f1s_sem,
    f1r_sem,
    f2s_sem,
    f2r_sem,
):
    n = lax.axis_size("sp")
    sp, tp = lax.axis_index("sp"), lax.axis_index("tp")
    z, y = sp // 2, sp % 2
    pair, zz = z // 2, z % 2
    x, c = tp // 2, tp % 2
    length, w1 = vs.shape
    w2 = vl.shape[1]
    width = w1 + w2
    planes = flat.shape[1]
    state = planes // 4
    heads1, heads2 = steps_s.shape[0], steps_l.shape[0]
    halo = xbuf.shape[0] - length
    rows, units = gate_m.shape
    cols = down_m.shape[1]
    half = wg.shape[1]
    lift = units - half
    own = resid.shape[0]
    tokens = nall.shape[0]
    model = nall.shape[1]
    inner = jnp.where(pair != zz, 1, 0) == 1
    dz = 1 - 2 * pair

    def at(zi, yi):
        return (zi * 2 + yi, tp)

    mate_z = at(z + 1 - 2 * zz, y)
    mate_y = at(z, 1 - y)
    mate_x = (sp, (1 - x) * 2 + c)
    mate_c = (sp, x * 2 + 1 - c)

    def remote(src, dst, send, recv, device):
        return pltpu.make_async_remote_copy(
            src_ref=src, dst_ref=dst, send_sem=send, recv_sem=recv, device_id=device, device_id_type=MESH
        )

    barrier = pltpu.get_barrier_semaphore()
    peers = [(lax.rem(sp + k, n), tp) for k in range(1, n)] + [mate_x, mate_c]
    for peer in peers:
        pl.semaphore_signal(barrier, inc=1, device_id=peer, device_id_type=MESH)
    loads = []
    for src, dst in (
        (vs, xbuf.at[pl.ds(halo, length), pl.ds(0, w1)]),
        (vl, xbuf.at[pl.ds(halo, length), pl.ds(w1, w2)]),
        (flat, xbuf.at[pl.ds(halo, length), pl.ds(width, planes)]),
        (gs, gbuf.at[:, pl.ds(0, w1)]),
        (gl, gbuf.at[:, pl.ds(w1, w2)]),
        (proj_s, pbuf.at[pl.ds(0, w1), :]),
        (proj_l, pbuf.at[pl.ds(w1, w2), :]),
        (resid, rbuf),
    ):
        copy = pltpu.make_async_copy(src, dst, lsem.at[len(loads)])
        copy.start()
        loads.append(copy)
    pl.semaphore_wait(barrier, len(peers))

    halos = []
    for i, (src, lo, size) in enumerate(((vs, 0, w1), (vl, w1, w2), (flat, width, planes))):
        halos.append(
            remote(
                src.at[pl.ds(length - halo, halo), :],
                xbuf.at[pl.ds(0, halo), pl.ds(lo, size)],
                hs_sem.at[i],
                hr_sem.at[i],
                (lax.rem(sp + 1, n), tp),
            )
        )

    @pl.when(sp < n - 1)
    def _():
        for copy in halos:
            copy.start()

    def source(p, h):
        cut = pl.ds(pl.multiple_of(h * lift, LANE), half)
        return (gate_m.at[:, cut], up_m.at[:, cut], down_m.at[cut, :])[p]

    def place(p, b):
        if p == 2:
            return wd.at[b]
        return (wg, wu)[p].at[pl.ds(pl.multiple_of(b * rows, rows), rows), :]

    def weight_wait(p, b):
        remote(place(p, b), place(p, b), ws_sem.at[0, 0], wr_sem.at[p, b], mate_y).wait_recv()

    keep = [pltpu.make_async_copy(source(p, zz), place(p, sp), wl_sem.at[p]) for p in range(3)]
    other = [
        remote(source(p, 1 - zz), place(p, sp), ws_sem.at[0, p], wr_sem.at[p, sp], at(z + dz, y)) for p in range(3)
    ]
    same = [
        remote(source(p, zz), place(p, sp), ws_sem.at[1, p], wr_sem.at[p, sp], at(z + 2 * dz, y)) for p in range(3)
    ]
    outer_z = jnp.clip(z - dz, 0, 3)
    back = [
        remote(source(p, 1 - zz), place(p, sp), ws_sem.at[2, p], wr_sem.at[p, sp], at(outer_z, y)) for p in range(3)
    ]
    near = (2 * pair + 1 - zz) * 2 + y
    relay = [
        remote(place(p, near), place(p, near), ws_sem.at[3, p], wr_sem.at[p, near], at(z + 2 * dz, y))
        for p in range(3)
    ]
    across = [
        remote(source(p, zz), place(p, sp), wy_sem.at[0, p], wr_sem.at[p, sp], mate_y) for p in range(3)
    ]
    line = [near, (2 - pair) * 2 + y, (3 - 3 * pair) * 2 + y]
    spread = [
        [
            remote(place(p, b), place(p, b), wy_sem.at[1 + j, p], wr_sem.at[p, b], mate_y)
            for p in range(3)
        ]
        for j, b in enumerate(line)
    ]

    def start_line(p):
        other[p].start()

        @pl.when(inner)
        def _():
            back[p].start()

    def service(j, p):
        weight_wait(p, line[j])
        spread[j][p].start()
        if j == 0:

            @pl.when(inner)
            def _():
                relay[p].start()

    start_line(0)
    for copy in keep:
        copy.start()

    hrow[...] = jnp.zeros_like(hrow)
    srow[...] = jnp.zeros_like(srow)
    raw_s = steps_s[...].astype(F32)
    raw_l = steps_l[...].astype(F32)
    srow[0:heads1, :] = jnp.maximum(raw_s, 0.0) + jnp.log1p(jnp.exp(-jnp.abs(raw_s)))
    srow[heads1 : heads1 + heads2, :] = jnp.maximum(raw_l, 0.0) + jnp.log1p(jnp.exp(-jnp.abs(raw_l)))
    for h in range(heads1 + heads2):
        rate = rates_s[h] if h < heads1 else rates_l[h - heads1]
        offset = offs_s[h : h + 1, :] if h < heads1 else offs_l[h - heads1 : h - heads1 + 1, :]
        hrow[h : h + 1, :] = offset - jnp.exp(jnp.full((1, length), rate, F32)) * srow[h : h + 1, :]
    chunks = length // LANE
    ri = lax.broadcasted_iota(jnp.int32, (LANE, LANE), 0)
    ci = lax.broadcasted_iota(jnp.int32, (LANE, LANE), 1)
    upper = jnp.where(ri <= ci, 1.0, 0.0).astype(F32)
    slab = hrow.shape[0]
    stacked = jnp.concatenate([hrow[:, k * LANE : (k + 1) * LANE] for k in range(chunks)], axis=0)
    sums = lax.dot_general(
        stacked, upper, (((1,), (0,)), ((), ())), precision=HIGH, preferred_element_type=F32
    )
    base = jnp.zeros((slab, 1), F32)
    fill = jnp.zeros((LANE - 2 * slab, LANE), F32)
    for k in range(chunks):
        w = sums[k * slab : (k + 1) * slab] + base
        base = w[:, LANE - 1 : LANE]
        cut = slice(k * LANE, (k + 1) * LANE)
        wrow[:, cut] = w
        wcol[cut, :] = jnp.concatenate([w, srow[:, cut], fill], axis=0).T

    for copy in loads[:3]:
        copy.wait()

    @pl.when(sp > 0)
    def _():
        for copy in halos:
            copy.wait_recv()

    @pl.when(sp == 0)
    def _():
        xbuf[0:halo, :] = jnp.zeros((halo, width + planes), BF)

    def conv(lo, taps):
        wide = xbuf[:, lo : lo + LANE].astype(F32)
        total = wide * taps[-1]
        for k in range(len(taps) - 1):
            total = total + taps[k] * pltpu.roll(wide, len(taps) - 1 - k, 0)
        total = total[halo:]
        return total * jax.nn.sigmoid(total)

    count = taps_s.shape[0]
    for i in range(4):
        taps = [taps_m[k, i : i + 1, :].astype(F32) for k in range(count)]
        maps[:, i * LANE : (i + 1) * LANE] = conv(width + i * LANE, taps).astype(BF)
    lane = lax.broadcasted_iota(jnp.int32, (1, LANE), 1)
    size1, size2 = w1 // heads1, w2 // heads2

    def tile_heads(j):
        if j * LANE < w1:
            return [j * LANE // size1 + i for i in range(LANE // size1)], size1
        return [heads1 + (j * LANE - w1) // size2], size2

    def by_head(values, size):
        total = values[-1]
        for i in reversed(range(len(values) - 1)):
            total = jnp.where(lane < (i + 1) * size, values[i], total)
        return total

    def spread_cols(j, offset):
        own_heads, size = tile_heads(j)
        return by_head(
            [jnp.broadcast_to(wcol[:, offset + h : offset + h + 1], (length, LANE)) for h in own_heads], size
        )

    tiles = width // LANE
    slot = 0
    slots = {}
    for j in range(tiles):
        lo = j * LANE
        ref, at_lo = (taps_s, lo) if lo < w1 else (taps_l, lo - w1)
        taps = [ref[k : k + 1, at_lo : at_lo + LANE].astype(F32) for k in range(count)]
        driven = conv(lo, taps) * spread_cols(j, slab)
        own_heads, size = tile_heads(j)
        last = by_head([jnp.broadcast_to(wrow[h : h + 1, length - 1 : length], (1, LANE)) for h in own_heads], size)
        within = spread_cols(j, 0)
        late[:, lo : lo + LANE] = (driven * jnp.exp(last - within)).astype(BF)
        run[state : state + 1, lo : lo + LANE] = jnp.exp(last)
        for i, h in enumerate(own_heads):
            keep_lanes = driven
            if len(own_heads) > 1:
                keep_lanes = jnp.where((lane >= i * size) & (lane < (i + 1) * size), driven, 0.0)
            drv[:, slot * LANE : (slot + 1) * LANE] = keep_lanes.astype(BF)
            slots[h] = slot
            slot += 1

    for kind, lo, size in ((0, 0, w1), (1, w1, w2)):
        keys = maps[:, 2 * kind * LANE : (2 * kind + 1) * LANE]
        run[0:state, lo : lo + size] = lax.dot_general(
            keys, late[:, lo : lo + size], (((0,), (0,)), ((), ())), preferred_element_type=F32
        )
    lo_y, hi_y = state + 8, 2 * state + 8
    run[lo_y:hi_y, :] = jnp.zeros((state, width), F32)
    run[hi_y : hi_y + 1, :] = jnp.ones((1, width), F32)
    ahead = at(jnp.minimum(z + 1, 3), y)
    ahead2 = at(jnp.minimum(z + 2, 3), y)
    messages = [
        remote(smsg.at[0], rmsg.at[0], ms_sem.at[0], mr_sem.at[0], mate_y),
        remote(smsg.at[1], rmsg.at[1], ms_sem.at[1], mr_sem.at[1], ahead),
        remote(smsg.at[2], rmsg.at[2], ms_sem.at[2], mr_sem.at[2], ahead),
        remote(smsg.at[2], rmsg.at[2], ms_sem.at[3], mr_sem.at[2], ahead2),
    ]
    bridge = z == 1

    def write_state(k):
        smsg[k, 0:state, :] = run[0:state, :].astype(BF)
        smsg[k, state : state + 16, :] = jnp.broadcast_to(run[state : state + 1, :], (16, width)).astype(BF)

    def got_state(k):
        return rmsg[k, 0:state, :].astype(F32), rmsg[k, state : state + 1, :].astype(F32)

    def extend(got, decay):
        before = run[hi_y : hi_y + 1, :]
        run[lo_y:hi_y, :] = got * before + run[lo_y:hi_y, :]
        run[hi_y : hi_y + 1, :] = decay * before

    def put_before(got, decay):
        here = run[state : state + 1, :]
        run[0:state, :] = got * here + run[0:state, :]
        run[state : state + 1, :] = decay * here

    def take_row():
        messages[0].wait_recv()
        got, decay = got_state(0)

        @pl.when(y == 1)
        def _():
            extend(got, decay)
            put_before(got, decay)

        @pl.when(y == 0)
        def _():
            run[0:state, :] = run[0:state, :] * decay + got
            run[state : state + 1, :] = run[state : state + 1, :] * decay

        @pl.when(zz == 0)
        def _():
            write_state(1)
            messages[1].start()

    def take_half():
        @pl.when(zz == 1)
        def _():
            messages[1].wait_recv()
            got, decay = got_state(1)
            extend(got, decay)
            put_before(got, decay)

            @pl.when(bridge)
            def _():
                write_state(2)
                messages[2].start()
                messages[3].start()

    def take_rest():
        @pl.when(pair == 1)
        def _():
            messages[2].wait_recv()
            extend(*got_state(2))

    kinds = [[h for h in slots if h < heads1], [h for h in slots if h >= heads1]]

    def local_rows(i):
        r0 = i * LANE
        size_k = r0 + LANE
        rowid = lax.broadcasted_iota(jnp.int32, (LANE, size_k), 0) + r0
        colid = lax.broadcasted_iota(jnp.int32, (LANE, size_k), 1)
        mask = colid <= rowid
        for kind in range(2):
            keys = maps[0:size_k, 2 * kind * LANE : (2 * kind + 1) * LANE]
            reads = maps[r0 : r0 + LANE, (2 * kind + 1) * LANE : (2 * kind + 2) * LANE]
            scores = lax.dot_general(reads, keys, (((1,), (1,)), ((), ())), preferred_element_type=F32)
            for j in range(tiles):
                own_heads, _ = tile_heads(j)
                if own_heads[0] not in kinds[kind]:
                    continue
                total = None
                for h in own_heads:
                    spread_h = wcol[r0 : r0 + LANE, h : h + 1] - wrow[h : h + 1, 0:size_k]
                    mixing = (jnp.exp(jnp.where(mask, spread_h, -1e30)) * scores).astype(BF)
                    term = jnp.dot(
                        mixing,
                        drv[0:size_k, slots[h] * LANE : (slots[h] + 1) * LANE],
                        preferred_element_type=F32,
                    )
                    total = term if total is None else total + term
                loc[r0 : r0 + LANE, j * LANE : (j + 1) * LANE] = total

    write_state(0)
    messages[0].start()
    across[0].start()
    mark = (chunks + 1) // 2
    for i in range(mark):
        local_rows(i)
    take_row()
    start_line(1)
    across[1].start()
    for i in range(mark, chunks):
        local_rows(i)
    take_half()

    @pl.when(inner)
    def _():
        same[0].start()
        same[1].start()

    @pl.when(jnp.logical_not(inner))
    def _():
        other[2].start()

    service(0, 0)
    service(0, 1)

    @pl.when(jnp.logical_not(inner))
    def _():
        same[0].start()
        same[1].start()

    take_rest()

    for copy in loads[3:]:
        copy.wait()
    for j in range(tiles):
        lo = j * LANE
        kind = 0 if lo < w1 else 1
        own_heads, size = tile_heads(j)
        reads = maps[:, (2 * kind + 1) * LANE : (2 * kind + 2) * LANE]
        carry = run[state + 8 : 2 * state + 8, lo : lo + LANE].astype(BF)
        carried = jnp.dot(reads, carry, preferred_element_type=F32)
        scan_out = loc[:, lo : lo + LANE] + carried * jnp.exp(spread_cols(j, 0))
        gates = gbuf[:, lo : lo + LANE].astype(F32)
        gated = scan_out * (gates * jax.nn.sigmoid(gates))
        square = gated * gated
        scales = []
        for i in range(len(own_heads)):
            one = square
            if len(own_heads) > 1:
                one = jnp.where((lane >= i * size) & (lane < (i + 1) * size), square, 0.0)
            mean = jnp.sum(one, axis=1, keepdims=True) * (1.0 / size)
            scales.append(jnp.broadcast_to(lax.rsqrt(mean + head_eps), (length, LANE)))
        ref, at_lo = (gain_s, lo) if lo < w1 else (gain_l, lo - w1)
        gain = ref[0:1, at_lo : at_lo + LANE]
        hbuf[:, lo : lo + LANE] = (gated * by_head(scales, size) * gain).astype(BF)

    wide = 2 * LANE

    @pl.loop(0, model // wide)
    def _(i):
        cut = pl.ds(pl.multiple_of(i * wide, wide), wide)
        part[:, cut] = jnp.dot(hbuf[...], pbuf[:, cut], preferred_element_type=F32).astype(BF)

    def rows_of(xi, ci):
        return pl.ds(pl.multiple_of((xi * 2 + ci) * own, own), own)

    cores = [
        remote(part.at[rows_of(xi, 1 - c), :], d2d.at[i], ds_sem.at[i], dr_sem.at[i], mate_c)
        for i, xi in enumerate((1 - x, x))
    ]
    for copy in cores:
        copy.start()
    cores[0].wait_recv()
    xsend[...] = (part[rows_of(1 - x, c), :].astype(F32) + d2d[0].astype(F32)).astype(BF)
    cross = remote(xsend, xrecv, xs_sem.at[0], xr_sem.at[0], mate_x)
    cross.start()
    service(1, 0)
    cores[1].wait_recv()
    cross.wait_recv()
    mixed = part[rows_of(x, c), :].astype(F32) + d2d[1].astype(F32) + xrecv[...].astype(F32)
    middle = (rbuf[...].astype(F32) + mixed).astype(BF)
    mid[...] = middle
    broad = middle.astype(F32)
    scale = lax.rsqrt(jnp.mean(broad * broad, axis=-1, keepdims=True) + row_eps)

    def place_rows(zi, xi, ci):
        index = zi * 4 + ci * 2 + xi
        return index, nall.at[pl.ds(pl.multiple_of(index * own, own), own), :]

    _, my_rows = place_rows(zz, x, c)
    my_rows[...] = (broad * scale * cgain[...]).astype(BF)

    def share(i, zi, xi, ci, device):
        index, view = place_rows(zi, xi, ci)
        return remote(view, view, as_sem.at[i], ar_sem.at[index], device)

    def rows_wait(zi, xi, ci):
        share(0, zi, xi, ci, mate_c).wait_recv()

    shares = [
        share(0, zz, x, c, mate_x),
        share(1, zz, x, c, mate_z),
        share(2, zz, x, c, mate_c),
        share(3, zz, 1 - x, c, mate_c),
        share(4, 1 - zz, x, c, mate_x),
        share(5, 1 - zz, x, c, mate_c),
        share(6, 1 - zz, 1 - x, c, mate_c),
    ]
    for i in range(3):
        shares[i].start()

    @pl.when(inner)
    def _():
        other[2].start()
        back[2].start()

    same[2].start()

    @pl.when(inner)
    def _():
        weight_wait(2, near)
        relay[2].start()
        spread[0][2].start()

    across[2].start()
    service(1, 1)
    rows_wait(zz, 1 - x, c)
    shares[3].start()
    for p in range(2):
        service(2, p)
    rows_wait(1 - zz, x, c)
    shares[4].start()
    shares[5].start()

    for copy in keep:
        copy.wait()

    service(1, 2)

    far = [k * 2 + 1 - y for k in range(4)]
    for p in range(2):
        for b in far:
            weight_wait(p, b)
    rows_wait(zz, x, 1 - c)
    rows_wait(zz, 1 - x, 1 - c)
    hot = wide if half % wide == 0 else LANE
    first = zz * (2 * half - units)

    def up_rows(zi):
        span = pl.ds(pl.multiple_of(zi * (tokens // 2), tokens // 2), tokens // 2)

        @pl.loop(0, half // hot)
        def _(i):
            cut = pl.ds(pl.multiple_of(i * hot, hot), hot)
            have = nall[span, :]
            gate = jnp.dot(have, wg[:, cut], preferred_element_type=F32)
            up = jnp.dot(have, wu[:, cut], preferred_element_type=F32)
            unit = lax.broadcasted_iota(jnp.int32, (1, hot), 1) + i * hot
            value = gate * jax.nn.sigmoid(gate) * up
            hid[span, cut] = jnp.where(unit >= first, value, 0.0).astype(BF)

    up_rows(zz)
    rows_wait(1 - zz, 1 - x, c)
    shares[6].start()
    rows_wait(1 - zz, x, 1 - c)
    rows_wait(1 - zz, 1 - x, 1 - c)
    up_rows(1 - zz)

    order = [zi * 2 + yi for yi in (y, 1 - y) for zi in (3 * pair, 2 - pair, 1 + pair, 3 - 3 * pair)]
    known = [True] * 4 + [False] * 4
    z_first = [False] * (n - 2) + [True, False]
    core_rows = tokens // 4

    def strip(zi, ci):
        return pl.ds(pl.multiple_of(zi * (tokens // 2) + ci * core_rows, core_rows), core_rows)

    def swap(q):
        return [
            remote(
                psum.at[q, strip(zi, 1 - c), :],
                dcol.at[q, pl.ds(zi * core_rows, core_rows), :],
                p_sem.at[q, zi],
                q_sem.at[q, zi],
                mate_c,
            )
            for zi in range(2)
        ]

    def hop1(q):
        return remote(s1.at[q], r1.at[q], f1s_sem.at[q], f1r_sem.at[q], mate_z if z_first[q] else mate_x)

    def hop2(q):
        return remote(s2.at[q], r2.at[q], f2s_sem.at[q], f2r_sem.at[q], mate_x if z_first[q] else mate_z)

    def compute(q):
        if q == 2:

            @pl.when(jnp.logical_not(inner))
            def _():
                weight_wait(2, near)
                spread[0][2].start()

        if q == 3:
            service(2, 2)
        if not known[q]:
            weight_wait(2, order[q])

        @pl.loop(0, 4)
        def _(i):
            span = pl.ds(pl.multiple_of(i * core_rows, core_rows), core_rows)
            psum[q, span, :] = jnp.dot(
                hid[span, :], wd[order[q]], preferred_element_type=F32
            ).astype(BF)

        for copy in swap(q):
            copy.start()

    def sum1(q):
        for copy in swap(q):
            copy.wait_recv()
        for j in range(2):
            for send in (True, False):
                if z_first[q]:
                    zi, xi = (1 - zz if send else zz), j
                else:
                    zi, xi = j, (1 - x if send else x)
                a = pl.ds(pl.multiple_of(zi * (tokens // 2) + c * core_rows + xi * own, own), own)
                b = pl.ds(pl.multiple_of(zi * core_rows + xi * own, own), own)
                total = psum[q, a, :].astype(F32) + dcol[q, b, :].astype(F32)
                to = slice(j * own, (j + 1) * own)
                if send:
                    s1[q, to, :] = total.astype(BF)
                else:
                    k1[q, to, :] = total
        hop1(q).start()

    def sum2(q):
        hop1(q).wait_recv()
        second = x if z_first[q] else zz
        for send in (True, False):
            j = 1 - second if send else second
            cut = pl.ds(pl.multiple_of(j * own, own), own)
            total = k1[q, cut, :] + r1[q, cut, :].astype(F32)
            if send:
                s2[q] = total.astype(BF)
            else:
                k2[q] = total
        hop2(q).start()

    def sum3(q):
        hop2(q).wait_recv()
        cut = pl.ds(pl.multiple_of(order[q] * cols, cols), cols)
        out[:, cut] = (mid[:, cut].astype(F32) + k2[q] + r2[q].astype(F32)).astype(BF)

    stages = (compute, sum1, sum2, sum3)
    for step in range(n + len(stages) - 1):
        for i, stage in enumerate(stages):
            if 0 <= step - i < n:
                stage(step - i)

    @pl.when(sp < n - 1)
    def _():
        for copy in halos:
            copy.wait_send()

    messages[0].wait_send()

    @pl.when(zz == 0)
    def _():
        messages[1].wait_send()

    @pl.when(bridge)
    def _():
        messages[2].wait_send()
        messages[3].wait_send()

    for p in range(3):
        other[p].wait_send()
        same[p].wait_send()
        across[p].wait_send()
        for j in range(3):
            spread[j][p].wait_send()

        @pl.when(inner)
        def _(p=p):
            back[p].wait_send()
            relay[p].wait_send()

    for copy in cores + [cross] + shares:
        copy.wait_send()
    for q in range(n):
        for copy in swap(q) + [hop1(q), hop2(q)]:
            copy.wait_send()


def fused_layer(
    residual,
    small_value_inputs,
    large_value_inputs,
    small_gate_inputs,
    large_gate_inputs,
    state_projections,
    small_step_inputs,
    large_step_inputs,
    small_decay_offsets,
    large_decay_offsets,
    small_decay_rates,
    large_decay_rates,
    small_filter_taps,
    large_filter_taps,
    state_filter_taps,
    small_head_gains,
    large_head_gains,
    small_output_projection,
    large_output_projection,
    channel_norm_gain,
    gate_matrix,
    up_matrix,
    down_matrix,
):
    n = lax.axis_size("sp")
    length, w1 = small_value_inputs.shape
    w2 = large_value_inputs.shape[1]
    width = w1 + w2
    state = state_projections.shape[2]
    planes = state_projections.shape[1] * state
    heads = small_decay_rates.shape[0] + large_decay_rates.shape[0]
    rows, units = gate_matrix.shape
    cols = down_matrix.shape[1]
    own, model = residual.shape
    tiles = units // LANE
    half = (tiles + 1) // 2 * LANE
    halo = 16
    slab = 8 * ((heads + 7) // 8)
    tokens = 2 * length
    hops = 3
    vmem, dma = pltpu.VMEM, pltpu.SemaphoreType.DMA
    hbm = pl.BlockSpec(memory_space=pl.ANY)
    near = pl.BlockSpec(memory_space=pltpu.VMEM)
    scalar = pl.BlockSpec(memory_space=pltpu.SMEM)
    specs = [hbm] * 5 + [near] * 4 + [scalar] * 2 + [near] * 5 + [hbm] * 3 + [near] + [hbm] * 3
    scratch = [
        vmem((length + halo, width + planes), BF),
        vmem((length, width), BF),
        vmem((width, model), BF),
        vmem((own, model), BF),
        vmem((slab, length), F32),
        vmem((slab, length), F32),
        vmem((slab, length), F32),
        vmem((length, LANE), F32),
        vmem((length, planes), BF),
        vmem((length, heads * LANE), BF),
        vmem((length, width), BF),
        vmem((2 * state + 16, width), F32),
        vmem((hops, state + 16, width), BF),
        vmem((hops, state + 16, width), BF),
        vmem((length, width), F32),
        vmem((length, width), BF),
        vmem((length, model), BF),
        vmem((2, own, model), BF),
        vmem((own, model), BF),
        vmem((own, model), BF),
        vmem((own, model), BF),
        vmem((tokens, model), BF),
        vmem((tokens, half), BF),
        vmem((n * rows, half), BF),
        vmem((n * rows, half), BF),
        vmem((n, half, cols), BF),
        vmem((n, tokens, cols), BF),
        vmem((n, tokens // 2, cols), BF),
        vmem((n, 2 * own, cols), BF),
        vmem((n, 2 * own, cols), F32),
        vmem((n, 2 * own, cols), BF),
        vmem((n, own, cols), BF),
        vmem((n, own, cols), F32),
        vmem((n, own, cols), BF),
        dma((8,)),
        dma((3,)),
        dma((3,)),
        dma((4, 3)),
        dma((4, 3)),
        dma((3, n)),
        dma((3,)),
        dma((4,)),
        dma((3,)),
        dma((2,)),
        dma((2,)),
        dma((1,)),
        dma((1,)),
        dma((7,)),
        dma((8,)),
        dma((n, 2)),
        dma((n, 2)),
        dma((n,)),
        dma((n,)),
        dma((n,)),
        dma((n,)),
    ]
    return pl.pallas_call(
        fused_kernel,
        out_shape=jax.ShapeDtypeStruct((own, model), BF),
        in_specs=specs,
        out_specs=pl.BlockSpec(memory_space=pltpu.VMEM),
        scratch_shapes=scratch,
        compiler_params=pltpu.CompilerParams(
            collective_id=0, has_side_effects=True, vmem_limit_bytes=66 * 1024 * 1000
        ),
    )(
        small_value_inputs,
        large_value_inputs,
        small_gate_inputs,
        large_gate_inputs,
        state_projections.reshape(length, planes),
        small_step_inputs.T,
        large_step_inputs.T,
        small_decay_offsets.T,
        large_decay_offsets.T,
        small_decay_rates,
        large_decay_rates,
        small_filter_taps,
        large_filter_taps,
        state_filter_taps,
        small_head_gains.reshape(1, w1),
        large_head_gains.reshape(1, w2),
        small_output_projection,
        large_output_projection,
        residual,
        channel_norm_gain.reshape(1, model),
        gate_matrix,
        up_matrix,
        down_matrix,
    )


def solution(mesh):
    in_specs = (
        P(("sp", "tp"), None),
        P("sp", "tp"),
        P("sp", "tp"),
        P("sp", "tp"),
        P("sp", "tp"),
        P("sp", None, None),
        P("sp", "tp"),
        P("sp", "tp"),
        P("sp", "tp"),
        P("sp", "tp"),
        P("tp"),
        P("tp"),
        P(None, "tp"),
        P(None, "tp"),
        P(),
        P("tp"),
        P("tp"),
        P("tp", None),
        P("tp", None),
        P(),
        P("sp", "tp"),
        P("sp", "tp"),
        P("tp", "sp"),
    )

    def layer(*args):
        units = args[20].shape[1]
        if paired(mesh.shape["sp"], mesh.shape["tp"], units):
            return fused_layer(*args)
        return on_device(*args)

    return jax.shard_map(
        layer,
        mesh=mesh,
        in_specs=in_specs,
        out_specs=P(("sp", "tp"), None),
        check_vma=False,
    )
```

```python
import jax
import jax.numpy as jnp
from jax import lax
from jax.experimental import pallas as pl
from jax.experimental.pallas import tpu as pltpu
from jax.sharding import PartitionSpec as P


HIGH = lax.Precision.HIGHEST
head_eps = 1e-05
row_eps = 1e-06
BF = jnp.bfloat16
F32 = jnp.float32
MESH = pl.DeviceIdType.MESH
LANE = 128


def ring_order(n):
    ys = 1
    while ys * ys * 4 <= n:
        ys *= 2
    zs = n // ys
    if ys * zs != n or ys < 2 or zs % 2:
        return list(range(n))
    walk = []
    for z in range(zs):
        row = list(range(1, ys))
        walk += [z * ys + y for y in (row if z % 2 == 0 else row[::-1])]
    return walk + [z * ys for z in reversed(range(zs))]


def causal_conv(series, prior, taps):
    width, length = taps.shape[0], series.shape[0]
    padded = jnp.concatenate([prior, series], axis=0).astype(F32)
    total = jnp.zeros(series.shape, F32)
    for offset in range(width):
        total = total + taps[offset].astype(F32)[None, :] * padded[offset : offset + length]
    return jax.nn.silu(total)


def local_heads(conv_values, step, within, keys, reads):
    length, width = conv_values.shape
    heads = step.shape[1]
    size = width // heads
    driven = conv_values.reshape(length, heads, size) * step[:, :, None]
    scores = lax.dot_general(reads, keys, (((1,), (1,)), ((), ())), preferred_element_type=F32)
    mask = jnp.tril(jnp.ones((length, length), dtype=bool))
    outs, finals = [], []
    for h in range(heads):
        own = within[:, h]
        spread = jnp.where(mask, own[:, None] - own[None, :], 0.0)
        mixing = jnp.where(mask, jnp.exp(spread) * scores, 0.0).astype(BF)
        value = driven[:, h]
        outs.append(jnp.dot(mixing, value.astype(BF), preferred_element_type=F32))
        late = (value * jnp.exp(own[-1] - own)[:, None]).astype(BF)
        finals.append(
            lax.dot_general(late, keys, (((0,), (0,)), ((), ())), preferred_element_type=F32)
        )
    return outs, jnp.concatenate(finals, axis=0)


def finish_heads(outs, incoming, within, reads, gate_inputs, gains):
    size = outs[0].shape[1]
    done = []
    carried = lax.dot_general(
        reads, incoming.astype(BF), (((1,), (1,)), ((), ())), preferred_element_type=F32
    )
    for h, local in enumerate(outs):
        cols = slice(h * size, (h + 1) * size)
        scan_out = local + carried[:, cols] * jnp.exp(within[:, h])[:, None]
        gated = scan_out * jax.nn.silu(gate_inputs[:, cols].astype(F32))
        scale = lax.rsqrt(jnp.mean(gated * gated, axis=-1, keepdims=True) + head_eps)
        done.append((gated * scale * gains[cols][None, :]).astype(BF))
    return jnp.concatenate(done, axis=1)


def row_norm(rows, gain):
    wide = rows.astype(F32)
    scale = lax.rsqrt(jnp.mean(wide * wide, axis=-1, keepdims=True) + row_eps)
    return (wide * scale * gain[None, :]).astype(BF)


def ring_gather(own):
    n = lax.axis_size("sp")
    order = ring_order(n)
    place = [order.index(i) for i in range(n)]
    me = lax.axis_index("sp")
    at = jnp.asarray(place, jnp.int32)[me]
    owners = jnp.asarray(order, jnp.int32)
    ahead = [(order[i], order[(i + 1) % n]) for i in range(n)]
    back = [(b, a) for a, b in ahead]
    rows = own.shape[0]
    whole = jnp.zeros((n * rows,) + own.shape[1:], own.dtype)
    whole = lax.dynamic_update_slice(whole, own, (me * rows, 0))
    up = down = own
    half = n // 2
    for k in range(1, half + 1):
        from_up = owners[(at - k) % n] * rows
        from_down = owners[(at + k) % n] * rows
        if 2 * k == n:
            cut = rows // 2
            up, down = up[:cut], down[cut:]
            from_down = from_down + cut
        up = lax.ppermute(up, "sp", ahead)
        down = lax.ppermute(down, "sp", back)
        whole = lax.dynamic_update_slice(whole, up, (from_up, 0))
        whole = lax.dynamic_update_slice(whole, down, (from_down, 0))
    return whole


def on_device(
    residual,
    small_value_inputs,
    large_value_inputs,
    small_gate_inputs,
    large_gate_inputs,
    state_projections,
    small_step_inputs,
    large_step_inputs,
    small_decay_offsets,
    large_decay_offsets,
    small_decay_rates,
    large_decay_rates,
    small_filter_taps,
    large_filter_taps,
    state_filter_taps,
    small_head_gains,
    large_head_gains,
    small_output_projection,
    large_output_projection,
    channel_norm_gain,
    gate_matrix,
    up_matrix,
    down_matrix,
):
    n = lax.axis_size("sp")
    me = lax.axis_index("sp")
    margin = state_filter_taps.shape[0] - 1
    length, w1 = small_value_inputs.shape
    w2 = large_value_inputs.shape[1]
    state = state_projections.shape[2]
    planes = state_projections.shape[1] * state
    units = gate_matrix.shape[1]
    flat = state_projections.reshape(length, planes)
    series = jnp.concatenate([small_value_inputs, large_value_inputs, flat], axis=1)
    prior = lax.ppermute(
        series[length - margin :], "sp", [(i, i + 1) for i in range(n - 1)]
    )
    pack = jnp.concatenate([gate_matrix, up_matrix, down_matrix.T], axis=1)
    pack, prior = lax.optimization_barrier((pack, prior))
    whole = ring_gather(pack)

    taps = jnp.concatenate(
        [small_filter_taps, large_filter_taps, state_filter_taps.reshape(margin + 1, planes)], axis=1
    )
    conv = causal_conv(series, prior, taps)
    maps = conv[:, w1 + w2 :].astype(BF)
    keys1, reads1, keys2, reads2 = (maps[:, i * state : (i + 1) * state] for i in range(4))

    heads1 = small_decay_rates.shape[0]
    step = jax.nn.softplus(
        jnp.concatenate([small_step_inputs, large_step_inputs], axis=1).astype(F32)
    )
    rates = jnp.concatenate([small_decay_rates, large_decay_rates])
    offsets = jnp.concatenate([small_decay_offsets, large_decay_offsets], axis=1)
    log_decay = -jnp.exp(rates)[None, :] * step + offsets
    lower = jnp.tril(jnp.ones((length, length), F32))
    within = jnp.dot(lower, log_decay, precision=HIGH)

    outs1, final1 = local_heads(conv[:, :w1], step[:, :heads1], within[:, :heads1], keys1, reads1)
    outs2, final2 = local_heads(
        conv[:, w1 : w1 + w2], step[:, heads1:], within[:, heads1:], keys2, reads2
    )
    heads = rates.shape[0]
    total = jnp.exp(within[-1])
    row = jnp.pad(total[None, :], ((0, 15), (0, state - heads)))
    sent = jnp.concatenate([final1, final2, row], axis=0).astype(BF)
    gathered = lax.all_gather(sent, "sp").astype(F32)
    states1 = gathered[:, :w1].reshape(n, heads1, w1 // heads1, state)
    states2 = gathered[:, w1 : w1 + w2].reshape(n, heads - heads1, w2 // (heads - heads1), state)
    totals = gathered[:, w1 + w2, :heads]
    carry1, carry2 = jnp.zeros_like(states1[0]), jnp.zeros_like(states2[0])
    for hop in range(n - 1):
        factor1 = totals[hop, :heads1][:, None, None]
        factor2 = totals[hop, heads1:][:, None, None]
        carry1 = jnp.where(hop < me, carry1 * factor1 + states1[hop], carry1)
        carry2 = jnp.where(hop < me, carry2 * factor2 + states2[hop], carry2)
    carry1, carry2 = carry1.reshape(w1, state), carry2.reshape(w2, state)

    heads_small = finish_heads(
        outs1, carry1, within[:, :heads1], reads1, small_gate_inputs, small_head_gains
    )
    heads_large = finish_heads(
        outs2, carry2, within[:, heads1:], reads2, large_gate_inputs, large_head_gains
    )
    mixed = (
        jnp.dot(heads_small, small_output_projection, preferred_element_type=F32)
        + jnp.dot(heads_large, large_output_projection, preferred_element_type=F32)
    ).astype(BF)
    mixed = lax.psum_scatter(
        mixed,
        "tp",
        scatter_dimension=0,
        tiled=True,
    ).astype(F32)
    middle = (residual.astype(F32) + mixed).astype(BF)
    normed = row_norm(middle, channel_norm_gain)
    normed_all = lax.all_gather(normed, "tp", axis=0, tiled=True)
    gate = jnp.dot(normed_all, whole[:, :units], preferred_element_type=F32)
    up = jnp.dot(normed_all, whole[:, units : 2 * units], preferred_element_type=F32)
    hidden = (jax.nn.silu(gate) * up).astype(BF)
    partial = lax.dot_general(
        hidden, whole[:, 2 * units :], (((1,), (1,)), ((), ())), preferred_element_type=F32
    )
    down = lax.psum_scatter(
        partial.astype(BF), "tp", scatter_dimension=0, tiled=True
    ).astype(F32)
    return (middle.astype(F32) + down).astype(BF)


def geometry(n):
    ys = 1
    while ys * ys * 4 <= n:
        ys *= 2
    return ys, n // ys


def paired(n, tp, units):
    ys, zs = geometry(n)
    return ys == 2 and zs == 4 and tp == 4 and units % (2 * LANE) == LANE


def fused_kernel(
    vs,
    vl,
    gs,
    gl,
    flat,
    steps_s,
    steps_l,
    offs_s,
    offs_l,
    rates_s,
    rates_l,
    taps_s,
    taps_l,
    taps_m,
    gain_s,
    gain_l,
    proj_s,
    proj_l,
    resid,
    cgain,
    gate_m,
    up_m,
    down_m,
    out,
    xbuf,
    gbuf,
    pbuf,
    rbuf,
    hrow,
    srow,
    wrow,
    wcol,
    maps,
    drv,
    late,
    run,
    smsg,
    rmsg,
    loc,
    hbuf,
    part,
    d2d,
    xsend,
    xrecv,
    mid,
    nall,
    hid,
    wg,
    wu,
    wd,
    seams,
    seam_gate,
    seam_up,
    psum,
    dcol,
    s1,
    k1,
    r1,
    s2,
    k2,
    r2,
    lsem,
    hs_sem,
    hr_sem,
    ws_sem,
    wy_sem,
    wr_sem,
    wl_sem,
    ms_sem,
    mr_sem,
    ds_sem,
    dr_sem,
    xs_sem,
    xr_sem,
    as_sem,
    ar_sem,
    p_sem,
    q_sem,
    f1s_sem,
    f1r_sem,
    f2s_sem,
    f2r_sem,
):
    n = lax.axis_size("sp")
    sp, tp = lax.axis_index("sp"), lax.axis_index("tp")
    z, y = sp // 2, sp % 2
    pair, zz = z // 2, z % 2
    x, c = tp // 2, tp % 2
    length, w1 = vs.shape
    w2 = vl.shape[1]
    width = w1 + w2
    planes = flat.shape[1]
    state = planes // 4
    heads1, heads2 = steps_s.shape[0], steps_l.shape[0]
    halo = xbuf.shape[0] - length
    rows, units = gate_m.shape
    cols = down_m.shape[1]
    half = wg.shape[1]
    seam = LANE // 2
    main = half - LANE
    share_units = units // 2
    own = resid.shape[0]
    tokens = nall.shape[0]
    model = nall.shape[1]
    inner = jnp.where(pair != zz, 1, 0) == 1
    dz = 1 - 2 * pair

    def at(zi, yi):
        return (zi * 2 + yi, tp)

    mate_z = at(z + 1 - 2 * zz, y)
    mate_y = at(z, 1 - y)
    mate_x = (sp, (1 - x) * 2 + c)
    mate_c = (sp, x * 2 + 1 - c)

    def remote(src, dst, send, recv, device):
        return pltpu.make_async_remote_copy(
            src_ref=src, dst_ref=dst, send_sem=send, recv_sem=recv, device_id=device, device_id_type=MESH
        )

    barrier = pltpu.get_barrier_semaphore()
    peers = [(lax.rem(sp + k, n), tp) for k in range(1, n)] + [mate_x, mate_c]
    for peer in peers:
        pl.semaphore_signal(barrier, inc=1, device_id=peer, device_id_type=MESH)
    loads = []
    for src, dst in (
        (vs, xbuf.at[pl.ds(halo, length), pl.ds(0, w1)]),
        (vl, xbuf.at[pl.ds(halo, length), pl.ds(w1, w2)]),
        (flat, xbuf.at[pl.ds(halo, length), pl.ds(width, planes)]),
        (gs, gbuf.at[:, pl.ds(0, w1)]),
        (gl, gbuf.at[:, pl.ds(w1, w2)]),
        (proj_s, pbuf.at[pl.ds(0, w1), :]),
        (proj_l, pbuf.at[pl.ds(w1, w2), :]),
        (resid, rbuf),
    ):
        copy = pltpu.make_async_copy(src, dst, lsem.at[len(loads)])
        copy.start()
        loads.append(copy)
    tiles5 = [
        pltpu.make_async_copy(src.at[:, pl.ds(main, LANE)], dst, lsem.at[len(loads) + i])
        for i, (src, dst) in enumerate(((gate_m, seam_gate), (up_m, seam_up)))
    ]
    for copy in tiles5:
        copy.start()
    pl.semaphore_wait(barrier, len(peers))

    halos = []
    for i, (src, lo, size) in enumerate(((vs, 0, w1), (vl, w1, w2), (flat, width, planes))):
        halos.append(
            remote(
                src.at[pl.ds(length - halo, halo), :],
                xbuf.at[pl.ds(0, halo), pl.ds(lo, size)],
                hs_sem.at[i],
                hr_sem.at[i],
                (lax.rem(sp + 1, n), tp),
            )
        )

    @pl.when(sp < n - 1)
    def _():
        for copy in halos:
            copy.start()

    def lanes(start, size):
        return pl.ds(pl.multiple_of(start, LANE), size)

    def source(p, h):
        if p == 2:
            return down_m.at[pl.ds(pl.multiple_of(h * share_units, seam), share_units), :]
        if p == 3:
            return seams.at[h]
        return (gate_m, up_m)[p].at[:, lanes(h * half, main)]

    def place(p, b, h):
        if p == 2:
            return wd.at[b, pl.ds(pl.multiple_of(h * seam, seam), share_units), :]
        block = pl.ds(pl.multiple_of(b * rows, rows), rows)
        if p == 3:
            return wg.at[block, lanes((1 - h) * main, LANE)]
        return (wg, wu)[p].at[block, lanes(h * LANE, main)]

    def weight_wait(p, b):
        remote(place(p, b, zz), place(p, b, zz), ws_sem.at[0, 0], wr_sem.at[p, b], mate_y).wait_recv()

    pieces = range(4)
    groups = ((0,), (1, 3), (2,))
    keep = [pltpu.make_async_copy(source(p, zz), place(p, sp, zz), wl_sem.at[p]) for p in pieces]

    def own_sends(kind, h, device):
        return [
            remote(source(p, h), place(p, sp, h), ws_sem.at[kind, p], wr_sem.at[p, sp], device) for p in pieces
        ]

    other = own_sends(0, 1 - zz, at(z + dz, y))
    same = own_sends(1, zz, at(z + 2 * dz, y))
    back = own_sends(2, 1 - zz, at(jnp.clip(z - dz, 0, 3), y))
    near = (2 * pair + 1 - zz) * 2 + y
    relay = [
        remote(place(p, near, zz), place(p, near, zz), ws_sem.at[3, p], wr_sem.at[p, near], at(z + 2 * dz, y))
        for p in pieces
    ]
    across = [
        remote(source(p, zz), place(p, sp, zz), wy_sem.at[0, p], wr_sem.at[p, sp], mate_y) for p in pieces
    ]
    line = [near, (2 - pair) * 2 + y, (3 - 3 * pair) * 2 + y]
    spread = [
        [
            remote(place(p, b, zz), place(p, b, zz), wy_sem.at[1 + j, p], wr_sem.at[p, b], mate_y)
            for p in pieces
        ]
        for j, b in enumerate(line)
    ]

    def start(copies, g):
        for p in groups[g]:
            copies[p].start()

    def arrived(j, g):
        for p in groups[g]:
            weight_wait(p, line[j])

    def service(j, g):
        arrived(j, g)
        start(spread[j], g)

    def only(cond, *actions):
        @pl.when(cond)
        def _():
            for action, *args in actions:
                action(*args)

    outer = jnp.logical_not(inner)
    z0, z1, z2, z3 = [z == k for k in range(4)]

    only(inner, (start, same, 0), (start, other, 0), (start, back, 0))
    only(outer, (start, other, 0))
    for p in range(3):
        keep[p].start()
    for copy in tiles5:
        copy.wait()
    left = lax.broadcasted_iota(jnp.int32, (1, LANE), 1) < seam
    turned = pltpu.roll(seam_up[...].astype(F32), seam, 1)
    plain = seam_gate[...].astype(F32)
    seams[0] = jnp.where(left, plain, turned).astype(BF)
    seams[1] = jnp.where(left, turned, plain).astype(BF)
    wu[:, lanes((1 - zz) * main, LANE)] = jnp.zeros((n * rows, LANE), BF)
    for b in range(n):
        wd[b, pl.ds(pl.multiple_of((1 - zz) * share_units, seam), seam), :] = jnp.zeros((seam, cols), BF)

    hrow[...] = jnp.zeros_like(hrow)
    srow[...] = jnp.zeros_like(srow)
    raw_s = steps_s[...].astype(F32)
    raw_l = steps_l[...].astype(F32)
    srow[0:heads1, :] = jnp.maximum(raw_s, 0.0) + jnp.log1p(jnp.exp(-jnp.abs(raw_s)))
    srow[heads1 : heads1 + heads2, :] = jnp.maximum(raw_l, 0.0) + jnp.log1p(jnp.exp(-jnp.abs(raw_l)))
    for h in range(heads1 + heads2):
        rate = rates_s[h] if h < heads1 else rates_l[h - heads1]
        offset = offs_s[h : h + 1, :] if h < heads1 else offs_l[h - heads1 : h - heads1 + 1, :]
        hrow[h : h + 1, :] = offset - jnp.exp(jnp.full((1, length), rate, F32)) * srow[h : h + 1, :]
    chunks = length // LANE
    ri = lax.broadcasted_iota(jnp.int32, (LANE, LANE), 0)
    ci = lax.broadcasted_iota(jnp.int32, (LANE, LANE), 1)
    upper = jnp.where(ri <= ci, 1.0, 0.0).astype(F32)
    slab = hrow.shape[0]
    stacked = jnp.concatenate([hrow[:, k * LANE : (k + 1) * LANE] for k in range(chunks)], axis=0)
    sums = lax.dot_general(
        stacked, upper, (((1,), (0,)), ((), ())), precision=HIGH, preferred_element_type=F32
    )
    base = jnp.zeros((slab, 1), F32)
    fill = jnp.zeros((LANE - 2 * slab, LANE), F32)
    for k in range(chunks):
        w = sums[k * slab : (k + 1) * slab] + base
        base = w[:, LANE - 1 : LANE]
        cut = slice(k * LANE, (k + 1) * LANE)
        wrow[:, cut] = w
        wcol[cut, :] = jnp.concatenate([w, srow[:, cut], fill], axis=0).T

    for copy in loads[:3]:
        copy.wait()

    @pl.when(sp > 0)
    def _():
        for copy in halos:
            copy.wait_recv()

    @pl.when(sp == 0)
    def _():
        xbuf[0:halo, :] = jnp.zeros((halo, width + planes), BF)

    def conv(lo, taps):
        wide = xbuf[:, lo : lo + LANE].astype(F32)
        total = wide * taps[-1]
        for k in range(len(taps) - 1):
            total = total + taps[k] * pltpu.roll(wide, len(taps) - 1 - k, 0)
        total = total[halo:]
        return total * jax.nn.sigmoid(total)

    count = taps_s.shape[0]
    for i in range(4):
        taps = [taps_m[k, i : i + 1, :].astype(F32) for k in range(count)]
        maps[:, i * LANE : (i + 1) * LANE] = conv(width + i * LANE, taps).astype(BF)
    lane = lax.broadcasted_iota(jnp.int32, (1, LANE), 1)
    size1, size2 = w1 // heads1, w2 // heads2

    def tile_heads(j):
        if j * LANE < w1:
            return [j * LANE // size1 + i for i in range(LANE // size1)], size1
        return [heads1 + (j * LANE - w1) // size2], size2

    def by_head(values, size):
        total = values[-1]
        for i in reversed(range(len(values) - 1)):
            total = jnp.where(lane < (i + 1) * size, values[i], total)
        return total

    def spread_cols(j, offset):
        own_heads, size = tile_heads(j)
        return by_head(
            [jnp.broadcast_to(wcol[:, offset + h : offset + h + 1], (length, LANE)) for h in own_heads], size
        )

    tiles = width // LANE
    slot = 0
    slots = {}
    for j in range(tiles):
        lo = j * LANE
        ref, at_lo = (taps_s, lo) if lo < w1 else (taps_l, lo - w1)
        taps = [ref[k : k + 1, at_lo : at_lo + LANE].astype(F32) for k in range(count)]
        driven = conv(lo, taps) * spread_cols(j, slab)
        own_heads, size = tile_heads(j)
        last = by_head([jnp.broadcast_to(wrow[h : h + 1, length - 1 : length], (1, LANE)) for h in own_heads], size)
        within = spread_cols(j, 0)
        late[:, lo : lo + LANE] = (driven * jnp.exp(last - within)).astype(BF)
        run[state : state + 1, lo : lo + LANE] = jnp.exp(last)
        for i, h in enumerate(own_heads):
            keep_lanes = driven
            if len(own_heads) > 1:
                keep_lanes = jnp.where((lane >= i * size) & (lane < (i + 1) * size), driven, 0.0)
            drv[:, slot * LANE : (slot + 1) * LANE] = keep_lanes.astype(BF)
            slots[h] = slot
            slot += 1

    for kind, lo, size in ((0, 0, w1), (1, w1, w2)):
        keys = maps[:, 2 * kind * LANE : (2 * kind + 1) * LANE]
        run[0:state, lo : lo + size] = lax.dot_general(
            keys, late[:, lo : lo + size], (((0,), (0,)), ((), ())), preferred_element_type=F32
        )
    lo_y, hi_y = state + 8, 2 * state + 8
    run[lo_y:hi_y, :] = jnp.zeros((state, width), F32)
    run[hi_y : hi_y + 1, :] = jnp.ones((1, width), F32)
    ahead = at(jnp.minimum(z + 1, 3), y)
    ahead2 = at(jnp.minimum(z + 2, 3), y)
    messages = [
        remote(smsg.at[0], rmsg.at[0], ms_sem.at[0], mr_sem.at[0], mate_y),
        remote(smsg.at[1], rmsg.at[1], ms_sem.at[1], mr_sem.at[1], ahead),
        remote(smsg.at[2], rmsg.at[2], ms_sem.at[2], mr_sem.at[2], ahead),
        remote(smsg.at[2], rmsg.at[2], ms_sem.at[3], mr_sem.at[2], ahead2),
    ]
    bridge = z == 1

    def write_state(k):
        smsg[k, 0:state, :] = run[0:state, :].astype(BF)
        smsg[k, state : state + 16, :] = jnp.broadcast_to(run[state : state + 1, :], (16, width)).astype(BF)

    def got_state(k):
        return rmsg[k, 0:state, :].astype(F32), rmsg[k, state : state + 1, :].astype(F32)

    def extend(got, decay):
        before = run[hi_y : hi_y + 1, :]
        run[lo_y:hi_y, :] = got * before + run[lo_y:hi_y, :]
        run[hi_y : hi_y + 1, :] = decay * before

    def put_before(got, decay):
        here = run[state : state + 1, :]
        run[0:state, :] = got * here + run[0:state, :]
        run[state : state + 1, :] = decay * here

    def take_row():
        messages[0].wait_recv()
        got, decay = got_state(0)

        @pl.when(y == 1)
        def _():
            extend(got, decay)
            put_before(got, decay)

        @pl.when(y == 0)
        def _():
            run[0:state, :] = run[0:state, :] * decay + got
            run[state : state + 1, :] = run[state : state + 1, :] * decay

        @pl.when(zz == 0)
        def _():
            write_state(1)
            messages[1].start()

    def take_half():
        @pl.when(zz == 1)
        def _():
            messages[1].wait_recv()
            got, decay = got_state(1)
            extend(got, decay)
            put_before(got, decay)

            @pl.when(bridge)
            def _():
                write_state(2)
                messages[2].start()
                messages[3].start()

    def take_rest():
        @pl.when(pair == 1)
        def _():
            messages[2].wait_recv()
            extend(*got_state(2))

    kinds = [[h for h in slots if h < heads1], [h for h in slots if h >= heads1]]

    def local_rows(i):
        r0 = i * LANE
        size_k = r0 + LANE
        rowid = lax.broadcasted_iota(jnp.int32, (LANE, size_k), 0) + r0
        colid = lax.broadcasted_iota(jnp.int32, (LANE, size_k), 1)
        mask = colid <= rowid
        for kind in range(2):
            keys = maps[0:size_k, 2 * kind * LANE : (2 * kind + 1) * LANE]
            reads = maps[r0 : r0 + LANE, (2 * kind + 1) * LANE : (2 * kind + 2) * LANE]
            scores = lax.dot_general(reads, keys, (((1,), (1,)), ((), ())), preferred_element_type=F32)
            for j in range(tiles):
                own_heads, _ = tile_heads(j)
                if own_heads[0] not in kinds[kind]:
                    continue
                total = None
                for h in own_heads:
                    spread_h = wcol[r0 : r0 + LANE, h : h + 1] - wrow[h : h + 1, 0:size_k]
                    mixing = (jnp.exp(jnp.where(mask, spread_h, -1e30)) * scores).astype(BF)
                    term = jnp.dot(
                        mixing,
                        drv[0:size_k, slots[h] * LANE : (slots[h] + 1) * LANE],
                        preferred_element_type=F32,
                    )
                    total = term if total is None else total + term
                loc[r0 : r0 + LANE, j * LANE : (j + 1) * LANE] = total

    write_state(0)
    messages[0].start()
    keep[3].start()
    start(across, 0)
    start(across, 1)

    only(z1, (start, back, 1))
    only(z2, (service, 0, 0), (start, relay, 0), (start, same, 1), (start, other, 1))
    only(z3, (start, other, 1))
    mark = (chunks + 1) // 2
    for i in range(mark):
        local_rows(i)
    take_row()
    only(z0, (start, other, 1))
    only(z2, (start, back, 1))
    for i in range(mark, chunks):
        local_rows(i)
    take_half()
    only(z1, (service, 0, 0), (start, relay, 0), (start, same, 1), (start, other, 1))
    only(inner, (service, 0, 1), (start, relay, 1))
    only(outer, (service, 0, 0), (start, other, 2))
    take_rest()

    for copy in loads[3:]:
        copy.wait()
    for j in range(tiles):
        lo = j * LANE
        kind = 0 if lo < w1 else 1
        own_heads, size = tile_heads(j)
        reads = maps[:, (2 * kind + 1) * LANE : (2 * kind + 2) * LANE]
        carry = run[state + 8 : 2 * state + 8, lo : lo + LANE].astype(BF)
        carried = jnp.dot(reads, carry, preferred_element_type=F32)
        scan_out = loc[:, lo : lo + LANE] + carried * jnp.exp(spread_cols(j, 0))
        gates = gbuf[:, lo : lo + LANE].astype(F32)
        gated = scan_out * (gates * jax.nn.sigmoid(gates))
        square = gated * gated
        scales = []
        for i in range(len(own_heads)):
            one = square
            if len(own_heads) > 1:
                one = jnp.where((lane >= i * size) & (lane < (i + 1) * size), square, 0.0)
            mean = jnp.sum(one, axis=1, keepdims=True) * (1.0 / size)
            scales.append(jnp.broadcast_to(lax.rsqrt(mean + head_eps), (length, LANE)))
        ref, at_lo = (gain_s, lo) if lo < w1 else (gain_l, lo - w1)
        gain = ref[0:1, at_lo : at_lo + LANE]
        hbuf[:, lo : lo + LANE] = (gated * by_head(scales, size) * gain).astype(BF)

    wide = 2 * LANE

    @pl.loop(0, model // wide)
    def _(i):
        cut = pl.ds(pl.multiple_of(i * wide, wide), wide)
        part[:, cut] = jnp.dot(hbuf[...], pbuf[:, cut], preferred_element_type=F32).astype(BF)

    def rows_of(xi, ci):
        return pl.ds(pl.multiple_of((xi * 2 + ci) * own, own), own)

    cores = [
        remote(part.at[rows_of(xi, 1 - c), :], d2d.at[i], ds_sem.at[i], dr_sem.at[i], mate_c)
        for i, xi in enumerate((1 - x, x))
    ]
    for copy in cores:
        copy.start()
    only(outer, (start, same, 0), (start, same, 1), (start, across, 2))
    cores[0].wait_recv()
    xsend[...] = (part[rows_of(1 - x, c), :].astype(F32) + d2d[0].astype(F32)).astype(BF)
    cross = remote(xsend, xrecv, xs_sem.at[0], xr_sem.at[0], mate_x)
    cross.start()
    service(1, 0)
    only(outer, (service, 2, 0))
    cores[1].wait_recv()
    cross.wait_recv()
    mixed = part[rows_of(x, c), :].astype(F32) + d2d[1].astype(F32) + xrecv[...].astype(F32)
    middle = (rbuf[...].astype(F32) + mixed).astype(BF)
    mid[...] = middle
    broad = middle.astype(F32)
    scale = lax.rsqrt(jnp.mean(broad * broad, axis=-1, keepdims=True) + row_eps)

    def place_rows(zi, xi, ci):
        index = zi * 4 + ci * 2 + xi
        return index, nall.at[pl.ds(pl.multiple_of(index * own, own), own), :]

    _, my_rows = place_rows(zz, x, c)
    my_rows[...] = (broad * scale * cgain[...]).astype(BF)

    def share(i, zi, xi, ci, device):
        index, view = place_rows(zi, xi, ci)
        return remote(view, view, as_sem.at[i], ar_sem.at[index], device)

    def rows_wait(zi, xi, ci):
        share(0, zi, xi, ci, mate_c).wait_recv()

    shares = [
        share(0, zz, x, c, mate_x),
        share(1, zz, x, c, mate_z),
        share(2, zz, x, c, mate_c),
        share(3, zz, 1 - x, c, mate_c),
        share(4, 1 - zz, x, c, mate_x),
        share(5, 1 - zz, x, c, mate_c),
        share(6, 1 - zz, 1 - x, c, mate_c),
    ]
    for i in range(3):
        shares[i].start()

    start(same, 2)
    only(inner, (start, other, 2), (start, back, 2), (arrived, 0, 2), (start, relay, 2), (start, across, 2))
    only(outer, (service, 0, 1))
    only(z2, (service, 2, 0))
    service(1, 1)
    only(outer, (service, 2, 1))
    rows_wait(zz, 1 - x, c)
    shares[3].start()
    only(z1, (service, 2, 0))
    rows_wait(1 - zz, x, c)
    shares[4].start()
    shares[5].start()
    only(inner, (service, 2, 1), (start, spread[0], 2))

    far = [k * 2 + 1 - y for k in range(4)]
    for copy in keep:
        copy.wait()
    for p in (0, 1, 3):
        for b in far:
            weight_wait(p, b)
    rows_wait(zz, x, 1 - c)
    rows_wait(zz, 1 - x, 1 - c)
    hot = wide if half % wide == 0 else LANE
    first = zz * seam
    shared = (1 - zz) * main
    turn = seam + (1 - zz) * (hot - 2 * seam)

    def up_rows(zi):
        span = pl.ds(pl.multiple_of(zi * (tokens // 2), tokens // 2), tokens // 2)

        @pl.loop(0, half // hot)
        def _(i):
            cut = pl.ds(pl.multiple_of(i * hot, hot), hot)
            have = nall[span, :]
            gate = jnp.dot(have, wg[:, cut], preferred_element_type=F32)
            up = jnp.dot(have, wu[:, cut], preferred_element_type=F32)
            unit = lax.broadcasted_iota(jnp.int32, (1, hot), 1) + i * hot
            up = jnp.where((unit >= shared) & (unit < shared + LANE), pltpu.roll(gate, turn, 1), up)
            value = gate * jax.nn.sigmoid(gate) * up
            used = (unit >= first) & (unit < first + share_units)
            hid[span, cut] = jnp.where(used, value, 0.0).astype(BF)

    up_rows(zz)

    service(1, 2)
    only(outer, (service, 0, 2))
    rows_wait(1 - zz, 1 - x, c)
    shares[6].start()
    rows_wait(1 - zz, x, 1 - c)
    rows_wait(1 - zz, 1 - x, 1 - c)
    up_rows(1 - zz)

    order = [zi * 2 + yi for yi in (y, 1 - y) for zi in (3 * pair, 2 - pair, 1 + pair, 3 - 3 * pair)]
    known = [True] * 4 + [False] * 4
    z_first = [q % 2 == 1 for q in range(n)]
    core_rows = tokens // 4

    def strip(zi, ci):
        return pl.ds(pl.multiple_of(zi * (tokens // 2) + ci * core_rows, core_rows), core_rows)

    def swap(q):
        return [
            remote(
                psum.at[q, strip(zi, 1 - c), :],
                dcol.at[q, pl.ds(zi * core_rows, core_rows), :],
                p_sem.at[q, zi],
                q_sem.at[q, zi],
                mate_c,
            )
            for zi in range(2)
        ]

    def hop1(q):
        return remote(s1.at[q], r1.at[q], f1s_sem.at[q], f1r_sem.at[q], mate_z if z_first[q] else mate_x)

    def hop2(q):
        return remote(s2.at[q], r2.at[q], f2s_sem.at[q], f2r_sem.at[q], mate_x if z_first[q] else mate_z)

    def compute(q):
        if q == 3:
            service(2, 2)
        if not known[q]:
            weight_wait(2, order[q])

        @pl.loop(0, 4)
        def _(i):
            span = pl.ds(pl.multiple_of(i * core_rows, core_rows), core_rows)
            psum[q, span, :] = jnp.dot(
                hid[span, :], wd[order[q]], preferred_element_type=F32
            ).astype(BF)

        for copy in swap(q):
            copy.start()

    def sum1(q):
        for copy in swap(q):
            copy.wait_recv()
        for j in range(2):
            for send in (True, False):
                if z_first[q]:
                    zi, xi = (1 - zz if send else zz), j
                else:
                    zi, xi = j, (1 - x if send else x)
                a = pl.ds(pl.multiple_of(zi * (tokens // 2) + c * core_rows + xi * own, own), own)
                b = pl.ds(pl.multiple_of(zi * core_rows + xi * own, own), own)
                total = psum[q, a, :].astype(F32) + dcol[q, b, :].astype(F32)
                to = slice(j * own, (j + 1) * own)
                if send:
                    s1[q, to, :] = total.astype(BF)
                else:
                    k1[q, to, :] = total
        hop1(q).start()

    def sum2(q):
        hop1(q).wait_recv()
        second = x if z_first[q] else zz
        for send in (True, False):
            j = 1 - second if send else second
            cut = pl.ds(pl.multiple_of(j * own, own), own)
            total = k1[q, cut, :] + r1[q, cut, :].astype(F32)
            if send:
                s2[q] = total.astype(BF)
            else:
                k2[q] = total
        hop2(q).start()

    def sum3(q):
        hop2(q).wait_recv()
        cut = pl.ds(pl.multiple_of(order[q] * cols, cols), cols)
        out[:, cut] = (mid[:, cut].astype(F32) + k2[q] + r2[q].astype(F32)).astype(BF)

    stages = ((sum1, 2), (sum2, 4), (compute, 0), (sum3, 6))
    for step in range(n + 6):
        for stage, lag in stages:
            if 0 <= step - lag < n:
                stage(step - lag)

    @pl.when(sp < n - 1)
    def _():
        for copy in halos:
            copy.wait_send()

    messages[0].wait_send()

    @pl.when(zz == 0)
    def _():
        messages[1].wait_send()

    @pl.when(bridge)
    def _():
        messages[2].wait_send()
        messages[3].wait_send()

    for p in pieces:
        other[p].wait_send()
        same[p].wait_send()
        across[p].wait_send()
        for j in range(3):
            spread[j][p].wait_send()

        @pl.when(inner)
        def _(p=p):
            back[p].wait_send()
            relay[p].wait_send()

    for copy in cores + [cross] + shares:
        copy.wait_send()
    for q in range(n):
        for copy in swap(q) + [hop1(q), hop2(q)]:
            copy.wait_send()


def fused_layer(
    residual,
    small_value_inputs,
    large_value_inputs,
    small_gate_inputs,
    large_gate_inputs,
    state_projections,
    small_step_inputs,
    large_step_inputs,
    small_decay_offsets,
    large_decay_offsets,
    small_decay_rates,
    large_decay_rates,
    small_filter_taps,
    large_filter_taps,
    state_filter_taps,
    small_head_gains,
    large_head_gains,
    small_output_projection,
    large_output_projection,
    channel_norm_gain,
    gate_matrix,
    up_matrix,
    down_matrix,
):
    n = lax.axis_size("sp")
    length, w1 = small_value_inputs.shape
    w2 = large_value_inputs.shape[1]
    width = w1 + w2
    state = state_projections.shape[2]
    planes = state_projections.shape[1] * state
    heads = small_decay_rates.shape[0] + large_decay_rates.shape[0]
    rows, units = gate_matrix.shape
    cols = down_matrix.shape[1]
    own, model = residual.shape
    tiles = units // LANE
    half = (tiles + 1) // 2 * LANE
    halo = 16
    slab = 8 * ((heads + 7) // 8)
    tokens = 2 * length
    hops = 3
    vmem, dma = pltpu.VMEM, pltpu.SemaphoreType.DMA
    hbm = pl.BlockSpec(memory_space=pl.ANY)
    near = pl.BlockSpec(memory_space=pltpu.VMEM)
    scalar = pl.BlockSpec(memory_space=pltpu.SMEM)
    specs = [hbm] * 5 + [near] * 4 + [scalar] * 2 + [near] * 5 + [hbm] * 3 + [near] + [hbm] * 3
    scratch = [
        vmem((length + halo, width + planes), BF),
        vmem((length, width), BF),
        vmem((width, model), BF),
        vmem((own, model), BF),
        vmem((slab, length), F32),
        vmem((slab, length), F32),
        vmem((slab, length), F32),
        vmem((length, LANE), F32),
        vmem((length, planes), BF),
        vmem((length, heads * LANE), BF),
        vmem((length, width), BF),
        vmem((2 * state + 16, width), F32),
        vmem((hops, state + 16, width), BF),
        vmem((hops, state + 16, width), BF),
        vmem((length, width), F32),
        vmem((length, width), BF),
        vmem((length, model), BF),
        vmem((2, own, model), BF),
        vmem((own, model), BF),
        vmem((own, model), BF),
        vmem((own, model), BF),
        vmem((tokens, model), BF),
        vmem((tokens, half), BF),
        vmem((n * rows, half), BF),
        vmem((n * rows, half), BF),
        vmem((n, half, cols), BF),
        vmem((2, rows, LANE), BF),
        vmem((rows, LANE), BF),
        vmem((rows, LANE), BF),
        vmem((n, tokens, cols), BF),
        vmem((n, tokens // 2, cols), BF),
        vmem((n, 2 * own, cols), BF),
        vmem((n, 2 * own, cols), F32),
        vmem((n, 2 * own, cols), BF),
        vmem((n, own, cols), BF),
        vmem((n, own, cols), F32),
        vmem((n, own, cols), BF),
        dma((10,)),
        dma((3,)),
        dma((3,)),
        dma((4, 4)),
        dma((4, 4)),
        dma((4, n)),
        dma((4,)),
        dma((4,)),
        dma((3,)),
        dma((2,)),
        dma((2,)),
        dma((1,)),
        dma((1,)),
        dma((7,)),
        dma((8,)),
        dma((n, 2)),
        dma((n, 2)),
        dma((n,)),
        dma((n,)),
        dma((n,)),
        dma((n,)),
    ]
    return pl.pallas_call(
        fused_kernel,
        out_shape=jax.ShapeDtypeStruct((own, model), BF),
        in_specs=specs,
        out_specs=pl.BlockSpec(memory_space=pltpu.VMEM),
        scratch_shapes=scratch,
        compiler_params=pltpu.CompilerParams(
            collective_id=0, has_side_effects=True, vmem_limit_bytes=66 * 1024 * 1000
        ),
    )(
        small_value_inputs,
        large_value_inputs,
        small_gate_inputs,
        large_gate_inputs,
        state_projections.reshape(length, planes),
        small_step_inputs.T,
        large_step_inputs.T,
        small_decay_offsets.T,
        large_decay_offsets.T,
        small_decay_rates,
        large_decay_rates,
        small_filter_taps,
        large_filter_taps,
        state_filter_taps,
        small_head_gains.reshape(1, w1),
        large_head_gains.reshape(1, w2),
        small_output_projection,
        large_output_projection,
        residual,
        channel_norm_gain.reshape(1, model),
        gate_matrix,
        up_matrix,
        down_matrix,
    )


def solution(mesh):
    in_specs = (
        P(("sp", "tp"), None),
        P("sp", "tp"),
        P("sp", "tp"),
        P("sp", "tp"),
        P("sp", "tp"),
        P("sp", None, None),
        P("sp", "tp"),
        P("sp", "tp"),
        P("sp", "tp"),
        P("sp", "tp"),
        P("tp"),
        P("tp"),
        P(None, "tp"),
        P(None, "tp"),
        P(),
        P("tp"),
        P("tp"),
        P("tp", None),
        P("tp", None),
        P(),
        P("sp", "tp"),
        P("sp", "tp"),
        P("tp", "sp"),
    )

    def layer(*args):
        units = args[20].shape[1]
        if paired(mesh.shape["sp"], mesh.shape["tp"], units):
            return fused_layer(*args)
        return on_device(*args)

    return jax.shard_map(
        layer,
        mesh=mesh,
        in_specs=in_specs,
        out_specs=P(("sp", "tp"), None),
        check_vma=False,
    )
```
